32 devices in a mesh: ep: 16 (over z, y, core), tp: 2 (over x).
Axes of the slice: x: 2, y: 2, z: 4, core: 2. Of those that a mesh axis runs over, the one named last changes fastest.
Arguments:
- tokens: bfloat16 [128, 1024], P(('ep', 'tp')), may hold values from -6 to 6
- lengths: int32 [128], P(('ep', 'tp')), may hold values from 256 to 1024, as said below
- cache_latent: bfloat16 [128, 1024, 256], P(('ep', 'tp')), may hold values from -160 to 160
- cache_rope: bfloat16 [128, 32, 1024], P(('ep', 'tp')), may hold values from -6 to 6
- attn_gain: float32 [1024], replicated, may hold values from 0.1 to 1.9
- latent_gain: float32 [256], replicated, may hold values from 0.1 to 1.9
- post_gain: float32 [1024], replicated, may hold values from 0.1 to 1.9
- ffn_gain: float32 [1024], replicated, may hold values from 0.1 to 1.9
- out_gain: float32 [1024], replicated, may hold values from 0.1 to 1.9
- w_latent: bfloat16 [1024, 256], P(None, 'tp'), may hold values from -0.1875 to 0.1875
- w_rope_key: bfloat16 [1024, 32], replicated, may hold values from -0.1875 to 0.1875
- w_query: bfloat16 [1024, 768], P(None, 'tp'), may hold values from -0.1875 to 0.1875
- w_absorb_key: bfloat16 [8, 64, 256], P('tp'), may hold values from -0.75 to 0.75
- w_absorb_value: bfloat16 [8, 256, 64], P('tp'), may hold values from -0.375 to 0.375
- w_out: bfloat16 [512, 1024], P('tp'), may hold values from -0.25 to 0.25
- routes: int32 [128, 6], P(('ep', 'tp')), may hold values from 0 to 15, all different within a row; in each aligned block of 8 rows (0 to 7, 8 to 15, ...) at most 5 rows name the same one
- route_weights: float32 [128, 6], P(('ep', 'tp')), may hold values from 0.2 to 1
- w_exp_gate: bfloat16 [16, 1024, 256], P('ep'), may hold values from -0.1875 to 0.1875
- w_exp_up: bfloat16 [16, 1024, 256], P('ep'), may hold values from -0.1875 to 0.1875
- w_exp_down: bfloat16 [16, 256, 1024], P('ep'), may hold values from -0.375 to 0.375
- w_dense_gate: bfloat16 [4096, 1024], P('ep'), may hold values from -0.1875 to 0.1875
- w_dense_up: bfloat16 [4096, 1024], P('ep'), may hold values from -0.1875 to 0.1875
- w_dense_down: bfloat16 [4096, 1024], P('ep'), may hold values from -0.09375 to 0.09375
- dense_gate_vector: float32 [1024], replicated, may hold values from -0.1875 to 0.1875
Outputs:
- output: bfloat16 [128, 1024], P(('ep', 'tp'))
- new_latent: bfloat16 [128, 256], P(('ep', 'tp'))
- new_rope_key: bfloat16 [128, 32], P(('ep', 'tp'))
The draws below stay inside these ranges and needn't reach their ends.
Inputs may be any that keep to these rules, and one draw needn't show every extreme that they name: `routes`: in each aligned block of 8 rows no expert is named by more than 5 rows; each row names 6 different experts. `lengths`: some sequence holds exactly 1024 cached positions.
All inputs are finite; a program needn't handle non-finite values.
Results may differ from the reference program's by a relative error of at most 0.015.
Values may be sent and summed in bfloat16 or wider, within the bound.
No kernel may reach another device: no remote copies, remote signals or barrier semaphores. Data moves between devices by JAX's collectives and lax.ppermute only.
A program may use at most 64 MiB of HBM per device.

```python
import math
import jax
import jax.numpy as jnp
import numpy as np
from jax import lax

D = 1024
HEADS = 8
NOPE = 64
ROPE = 32
V_HEAD = 64
KV_RANK = 256
EXPERT_FF = 256
SH_FF = 4096
TOPK = 6
CACHE_LEN = 1024
SEQ_GRP = 8
BATCH = 128
EXPERTS = 16
CAP = 5
N_EP = 16
N_TP = 2


def draw_lengths(key, part):
    first_key, second_key = jax.random.split(key)
    drawn = jax.random.randint(first_key, (BATCH,), CACHE_LEN // 4, CACHE_LEN + 1)
    chosen = jax.random.randint(second_key, (), 0, BATCH)
    return jnp.where(jnp.arange(BATCH) == chosen, CACHE_LEN, drawn).astype(jnp.int32)


def draw_cache_latent(key, part):
    keys = jax.random.split(key, 1)
    base = jnp.clip(jax.random.normal(keys[0], (BATCH, CACHE_LEN, KV_RANK), jnp.float32), -4.0, 4.0)
    return base.astype(jnp.bfloat16)


def block_levels(rng, shape, cuts, smallest, largest):
    def one(dim, blocks):
        draws = jax.random.uniform(jax.random.fold_in(jax.random.fold_in(rng, 6), dim), (blocks,), jnp.float32, smallest / len(cuts), largest / len(cuts))
        return jnp.repeat(jnp.exp(draws), shape[dim] // blocks).reshape((-1,) + (1,) * (len(shape) - dim - 1))

    level = one(*cuts[0])
    for cut in cuts[1:]:
        level = level * one(*cut)
    return level


def deal_out(key, own, number, rows, number_of, top, bound, skew):
    ranking = jax.random.permutation(key, number_of)
    packed, ordinary = load_shares(number_of, rows * top, bound, skew, True), load_shares(number_of, rows * top, bound, skew, False)
    places = jnp.arange(number_of)

    def named(sizes, rotation):
        used = int((sizes > 0).sum())
        fixed = max(1, used // 4)
        shifted = fixed + (places - fixed + rotation * (used - fixed)) % max(1, number_of - fixed)
        return jnp.zeros((number_of,), jnp.int32).at[ranking[jnp.where(places < fixed, places, shifted)]].set(jnp.asarray(sizes, jnp.int32))

    sizes = jnp.where(number % 4 == 0, named(packed, number // 4), named(ordinary, number - number // 4 - 1))
    mixed = jax.random.permutation(jax.random.fold_in(own, 3), number_of)
    source_of, sink = mixed[0:number_of // 2 * 2:2], mixed[1:number_of // 2 * 2:2]
    margin = jnp.minimum(sizes[source_of] - 1, bound - sizes[sink]) // 2
    margin = jnp.where((source_of == ranking[0]) | (sink == ranking[0]) | (sizes[sink] == 0), 0, jnp.maximum(margin, 0))
    shifted = jax.random.randint(jax.random.fold_in(own, 4), (number_of // 2,), 0, 1 << 20) % (margin + 1)
    sizes = sizes.at[source_of].add(-shifted).at[sink].add(shifted)
    items = jnp.searchsorted(jnp.cumsum(sizes), jnp.arange(rows * top), side="right").astype(jnp.int32)
    grid = items.reshape(top, rows).T
    grid = grid[jax.random.permutation(jax.random.fold_in(own, 1), rows)]
    rotation = jax.random.randint(jax.random.fold_in(own, 2), (rows, 1), 0, top)
    return jnp.take_along_axis(grid, (jnp.arange(top)[None, :] + rotation) % top, axis=1)


def load_shares(number_of, total, bound, lean, full):
    weights = [(1 << 20) // math.isqrt(standing ** lean) + 1 for standing in range(1, number_of + 1)]
    largest = bound if full else min(bound, max(-(-total // number_of), total * weights[0] // sum(weights)))
    least = 1 if total - largest >= number_of - 1 else 0
    holding, spare = [largest] + [least] * (number_of - 1), total - largest - least * (number_of - 1)
    while spare > 0:
        candidates = [i for i in range(1, number_of) if holding[i] < largest] or [i for i in range(1, number_of) if holding[i] < bound]
        whole, budget = sum([weights[i] for i in candidates]), spare
        for i in candidates:
            extra = min(bound - holding[i], max(1, budget * weights[i] // whole), spare)
            holding[i] = holding[i] + extra
            spare = spare - extra
    return np.array(holding)


def gaussian(stream_key, extent, scale, limit, cuts=(), kind=jnp.bfloat16):
    values = jax.random.normal(stream_key, extent, jnp.float32) * scale
    if len(cuts) > 0:
        values = block_levels(stream_key, extent, cuts, -0.22, 0.18) * values
    return jnp.clip(values, min=-limit, max=limit).astype(kind)


def setup_inputs(seed: int = 0) -> dict:
    arg_keys = jax.random.split(jax.random.key(seed), 25)
    tokens = gaussian(arg_keys[0], (BATCH, D), 1.0, 6.0, ((0, 32),))
    lengths = draw_lengths(jax.random.fold_in(arg_keys[24], 71), 0)
    cache_latent = draw_cache_latent(jax.random.fold_in(arg_keys[24], 71), 0)
    cache_rope = gaussian(arg_keys[3], (BATCH, ROPE, CACHE_LEN), 1.0, 6.0, ((0, 32),))
    attn_gain = jnp.clip(1.0 + 0.18 * jax.random.normal(arg_keys[4], (D,), jnp.float32), 0.1, 1.9)
    latent_gain = jnp.clip(1.0 + 0.18 * jax.random.normal(arg_keys[5], (KV_RANK,), jnp.float32), 0.1, 1.9)
    post_gain = jnp.clip(1.0 + 0.18 * jax.random.normal(arg_keys[6], (D,), jnp.float32), 0.1, 1.9)
    ffn_gain = jnp.clip(1.0 + 0.18 * jax.random.normal(arg_keys[7], (D,), jnp.float32), 0.1, 1.9)
    out_gain = jnp.clip(1.0 + 0.18 * jax.random.normal(arg_keys[8], (D,), jnp.float32), 0.1, 1.9)
    w_latent = gaussian(arg_keys[9], (D, KV_RANK), D ** -0.5, 0.1875, ((1, 2),))
    w_rope_key = gaussian(arg_keys[10], (D, ROPE), D ** -0.5, 0.1875)
    w_query = gaussian(arg_keys[11], (D, HEADS * (NOPE + ROPE)), D ** -0.5, 0.1875, ((1, 2),))
    w_absorb_key = gaussian(arg_keys[12], (HEADS, NOPE, KV_RANK), NOPE ** -0.5, 0.75, ((0, 2),))
    w_absorb_value = gaussian(arg_keys[13], (HEADS, KV_RANK, V_HEAD), KV_RANK ** -0.5, 0.375, ((0, 2),))
    w_out = gaussian(arg_keys[14], (HEADS * V_HEAD, D), (HEADS * V_HEAD) ** -0.5, 0.25, ((0, 2),))
    routes_keys = jax.random.split(jax.random.fold_in(arg_keys[15], 1), BATCH // SEQ_GRP)
    routes_turns = jax.random.permutation(jax.random.fold_in(arg_keys[15], 3), BATCH // SEQ_GRP)
    routes = jax.vmap(lambda own, number: deal_out(jax.random.fold_in(arg_keys[15], 2), own, number, SEQ_GRP, EXPERTS, TOPK, CAP, 2))(routes_keys, routes_turns).reshape((BATCH, TOPK))
    route_weights = jnp.clip(0.2 + 0.8 * jax.random.uniform(arg_keys[16], (BATCH, TOPK), jnp.float32) ** block_levels(arg_keys[16], (BATCH, TOPK), ((0, 32),), -0.2, 0.2), 0.2, 1.0)
    w_exp_gate = gaussian(arg_keys[17], (EXPERTS, D, EXPERT_FF), D ** -0.5, 0.1875, ((0, 16),))
    w_exp_up = gaussian(arg_keys[18], (EXPERTS, D, EXPERT_FF), D ** -0.5, 0.1875, ((0, 16),))
    w_exp_down = gaussian(arg_keys[19], (EXPERTS, EXPERT_FF, D), EXPERT_FF ** -0.5, 0.375, ((0, 16),))
    w_dense_gate = gaussian(arg_keys[20], (SH_FF, D), D ** -0.5, 0.1875, ((0, 16),))
    w_dense_up = gaussian(arg_keys[21], (SH_FF, D), D ** -0.5, 0.1875, ((0, 16),))
    w_dense_down = gaussian(arg_keys[22], (SH_FF, D), SH_FF ** -0.5, 0.09375, ((0, 16),))
    dense_gate_vector = gaussian(arg_keys[23], (D,), D ** -0.5, 0.1875, (), jnp.float32)
    return {"tokens": tokens, "lengths": lengths, "cache_latent": cache_latent, "cache_rope": cache_rope, "attn_gain": attn_gain, "latent_gain": latent_gain, "post_gain": post_gain, "ffn_gain": ffn_gain, "out_gain": out_gain, "w_latent": w_latent, "w_rope_key": w_rope_key, "w_query": w_query, "w_absorb_key": w_absorb_key, "w_absorb_value": w_absorb_value, "w_out": w_out, "routes": routes, "route_weights": route_weights, "w_exp_gate": w_exp_gate, "w_exp_up": w_exp_up, "w_exp_down": w_exp_down, "w_dense_gate": w_dense_gate, "w_dense_up": w_dense_up, "w_dense_down": w_dense_down, "dense_gate_vector": dense_gate_vector}


epsilon = 1e-06
rope_base = 10000.0
negative = -1e+30

def normalize(values, gain_vec):
    values = values.astype(jnp.float32)
    return values * lax.rsqrt(lax.optimization_barrier(jnp.mean(values * values, axis=-1, keepdims=True)) + epsilon) * gain_vec

def rotate(values, positions):
    half_width = values.shape[-1] // 2
    inverse = rope_base ** (-jnp.arange(half_width, dtype=jnp.float32) / half_width)
    angles = positions.astype(jnp.float32)[..., None] * inverse
    cosine = jnp.cos(angles)
    sine_part = jnp.sin(angles)
    first_half = values[..., :half_width]
    second = values[..., half_width:]
    return jnp.concatenate([first_half * cosine - second * sine_part, first_half * sine_part + second * cosine], axis=-1)

def attend(operands):
    q_latent, q_rope, cache_lat, cache_rot, new_lat, new_rot, seq_lengths = operands
    scaling = (NOPE + ROPE) ** (-0.5)
    scores = jnp.einsum('shc,slc->shl', q_latent.astype(jnp.float32), cache_lat.astype(jnp.float32))
    scores = scores + jnp.einsum('shr,srl->shl', q_rope.astype(jnp.float32), cache_rot.astype(jnp.float32))
    scores = scores * scaling
    own_score = lax.optimization_barrier(jnp.sum(q_latent.astype(jnp.float32) * new_lat.astype(jnp.float32)[:, None, :], axis=-1))
    own_score = (own_score + lax.optimization_barrier(jnp.sum(q_rope.astype(jnp.float32) * new_rot.astype(jnp.float32)[:, None, :], axis=-1))) * scaling
    visible = jnp.arange(cache_lat.shape[1], dtype=jnp.int32)[None, None, :] < seq_lengths[:, None, None]
    scores = jnp.where(visible, scores, negative)
    row_max = jnp.maximum(lax.optimization_barrier(jnp.max(scores, axis=-1)), own_score)
    weights = jnp.exp(scores - row_max[..., None])
    own_weight = jnp.exp(own_score - row_max)
    totals = lax.optimization_barrier(jnp.sum(weights, axis=-1)) + own_weight
    probabilities = (weights / totals[..., None]).astype(jnp.bfloat16)
    own_prob = (own_weight / totals).astype(jnp.bfloat16)
    mixed = jnp.einsum('shl,slc->shc', probabilities.astype(jnp.float32), cache_lat.astype(jnp.float32))
    mixed = mixed + own_prob.astype(jnp.float32)[..., None] * new_lat.astype(jnp.float32)[:, None, :]
    return mixed.astype(jnp.bfloat16)

def reference(tokens, lengths, cache_latent, cache_rope, attn_gain, latent_gain, post_gain, ffn_gain, out_gain, w_latent, w_rope_key, w_query, w_absorb_key, w_absorb_value, w_out, routes, route_weights, w_exp_gate, w_exp_up, w_exp_down, w_dense_gate, w_dense_up, w_dense_down, dense_gate_vector):
    hidden = normalize(tokens, attn_gain).astype(jnp.bfloat16)
    new_latent = normalize(jnp.dot(hidden, w_latent, preferred_element_type=jnp.float32), latent_gain).astype(jnp.bfloat16)
    new_rope_key = rotate(jnp.dot(hidden, w_rope_key, preferred_element_type=jnp.float32), lengths).astype(jnp.bfloat16)
    queries = jnp.dot(hidden, w_query, preferred_element_type=jnp.float32).astype(jnp.bfloat16)
    queries = queries.reshape(BATCH, HEADS, NOPE + ROPE)
    query_rope = rotate(queries[..., NOPE:].astype(jnp.float32), lengths[:, None]).astype(jnp.bfloat16)
    query_latent = jnp.einsum('shn,hnc->shc', queries[..., :NOPE].astype(jnp.float32), w_absorb_key.astype(jnp.float32)).astype(jnp.bfloat16)

    def grouped(array):
        return array.reshape((N_EP, SEQ_GRP) + array.shape[1:])
    attended = lax.map(attend, (grouped(query_latent), grouped(query_rope), grouped(cache_latent), grouped(cache_rope), grouped(new_latent), grouped(new_rope_key), grouped(lengths)))
    attended = attended.reshape(BATCH, HEADS, KV_RANK)
    head_out = jnp.einsum('shc,hcv->shv', attended.astype(jnp.float32), w_absorb_value.astype(jnp.float32)).astype(jnp.bfloat16)
    per_group = HEADS // N_TP
    pieces = jnp.einsum('sgk,gkd->sgd', head_out.reshape(BATCH, N_TP, per_group * V_HEAD).astype(jnp.float32), w_out.reshape(N_TP, per_group * V_HEAD, D).astype(jnp.float32))
    pieces = lax.optimization_barrier(pieces.astype(jnp.bfloat16))
    mixed = lax.optimization_barrier(jnp.sum(pieces.astype(jnp.float32), axis=1))
    residual = (tokens.astype(jnp.float32) + normalize(mixed, post_gain)).astype(jnp.bfloat16)
    ffn_in = normalize(residual, ffn_gain).astype(jnp.bfloat16)
    flattened = routes.reshape(N_EP, SEQ_GRP * TOPK)
    onehot = (flattened[..., None] == jnp.arange(EXPERTS, dtype=jnp.int32)).astype(jnp.int32)
    order_rank = lax.optimization_barrier(jnp.sum((jnp.cumsum(onehot, axis=1) - onehot) * onehot, axis=-1))
    slot_index = flattened * (N_EP * CAP) + jnp.arange(N_EP, dtype=jnp.int32)[:, None] * CAP + order_rank
    slot_index = slot_index.reshape(-1).astype(jnp.int32)
    repeated = jnp.repeat(ffn_in, TOPK, axis=0)
    buffer = jnp.zeros((EXPERTS * N_EP * CAP, D), jnp.bfloat16).at[slot_index].set(repeated)
    buffer = buffer.reshape(EXPERTS, N_EP * CAP, D)

    def expert(operands):
        rows_in, gate_w, up_w, down_w = operands
        gate_pre = jnp.dot(rows_in, gate_w, preferred_element_type=jnp.float32)
        up_proj = jnp.dot(rows_in, up_w, preferred_element_type=jnp.float32)
        activity = (jax.nn.silu(gate_pre) * up_proj).astype(jnp.bfloat16)
        return jnp.dot(activity, down_w, preferred_element_type=jnp.float32).astype(jnp.bfloat16)
    results = lax.map(expert, (buffer, w_exp_gate, w_exp_up, w_exp_down)).reshape(EXPERTS * N_EP * CAP, D)
    picked = results[slot_index.reshape(BATCH, TOPK)]
    routed = lax.optimization_barrier(jnp.sum(route_weights[..., None] * picked.astype(jnp.float32), axis=1))
    dense_pre = jnp.dot(ffn_in, w_dense_gate.T, preferred_element_type=jnp.float32)
    dense_up = jnp.dot(ffn_in, w_dense_up.T, preferred_element_type=jnp.float32)
    dense_act = (jax.nn.silu(dense_pre) * dense_up).astype(jnp.bfloat16)
    dense_out = jnp.dot(dense_act, w_dense_down, preferred_element_type=jnp.float32)
    dense_gate = jax.nn.sigmoid(lax.optimization_barrier(jnp.sum(ffn_in.astype(jnp.float32) * dense_gate_vector, axis=-1)))
    combined = routed + dense_gate[:, None] * dense_out
    output = (residual.astype(jnp.float32) + normalize(combined, out_gain)).astype(jnp.bfloat16)
    return (output, new_latent, new_rope_key)
```

```python
import jax
import jax.numpy as jnp
from jax import lax
from jax.sharding import PartitionSpec as P

epsilon = 1e-06
rope_base = 10000.0
negative = -1e30
f32 = jnp.float32
bf16 = jnp.bfloat16


def normalize(values, gain_vec):
    values = values.astype(f32)
    return (
        values * lax.rsqrt(jnp.mean(values * values, axis=-1, keepdims=True) + epsilon) * gain_vec
    )


def rotate(values, positions):
    half_width = values.shape[-1] // 2
    inverse = rope_base ** (-jnp.arange(half_width, dtype=f32) / half_width)
    angles = positions.astype(f32)[..., None] * inverse
    cosine = jnp.cos(angles)
    sine_part = jnp.sin(angles)
    first_half = values[..., :half_width]
    second = values[..., half_width:]
    return jnp.concatenate(
        [first_half * cosine - second * sine_part, first_half * sine_part + second * cosine],
        axis=-1,
    )


def split_float(values):
    high = lax.reduce_precision(values, 8, 7)
    return high.astype(bf16), (values - high).astype(bf16)


def join_float(high, low):
    return high.astype(f32) + low.astype(f32)


def shift(values, step, axis):
    count = lax.axis_size(axis)
    return lax.ppermute(values, axis, [(i, (i + step) % count) for i in range(count)])


def attend(q_latent, q_rope, cache_lat, cache_rot, new_lat, new_rot, seq_lengths, scaling):
    scores = jnp.einsum("shc,slc->shl", q_latent, cache_lat, preferred_element_type=f32)
    scores = scores + jnp.einsum("shr,srl->shl", q_rope, cache_rot, preferred_element_type=f32)
    scores = scores * scaling
    own_score = jnp.sum(q_latent.astype(f32) * new_lat.astype(f32)[:, None, :], axis=-1)
    own_score = (
        own_score + jnp.sum(q_rope.astype(f32) * new_rot.astype(f32)[:, None, :], axis=-1)
    ) * scaling
    visible = (
        jnp.arange(cache_lat.shape[1], dtype=jnp.int32)[None, None, :] < seq_lengths[:, None, None]
    )
    scores = jnp.where(visible, scores, negative)
    row_max = jnp.maximum(jnp.max(scores, axis=-1), own_score)
    weights = jnp.exp(scores - row_max[..., None])
    own_weight = jnp.exp(own_score - row_max)
    totals = jnp.sum(weights, axis=-1) + own_weight
    probabilities = (weights / totals[..., None]).astype(bf16)
    own_prob = (own_weight / totals).astype(bf16)
    mixed = jnp.einsum("shl,slc->shc", probabilities, cache_lat, preferred_element_type=f32)
    mixed = mixed + own_prob.astype(f32)[..., None] * new_lat.astype(f32)[:, None, :]
    return mixed.astype(bf16)


def shards(
    tokens,
    lengths,
    cache_latent,
    cache_rope,
    attn_gain,
    latent_gain,
    post_gain,
    ffn_gain,
    out_gain,
    w_latent,
    w_rope_key,
    w_query,
    w_absorb_key,
    w_absorb_value,
    w_out,
    routes,
    route_weights,
    w_exp_gate,
    w_exp_up,
    w_exp_down,
    w_dense_gate,
    w_dense_up,
    w_dense_down,
    dense_gate_vector,
):
    own_rows, model_width = tokens.shape
    tp_count = lax.axis_size("tp")
    ep_count = lax.axis_size("ep")
    me = lax.axis_index("tp")
    rope_width = w_rope_key.shape[1]
    local_heads, nope_width, rank = w_absorb_key.shape
    part = w_latent.shape[1]
    head_span = nope_width + rope_width
    scaling = head_span ** (-0.5)
    group_size = own_rows * tp_count

    rows = jnp.concatenate([tokens] + [shift(tokens, s, "tp") for s in range(1, tp_count)])
    hidden = normalize(rows, attn_gain).astype(bf16)
    new_rope_key = rotate(
        jnp.dot(hidden[:own_rows], w_rope_key, preferred_element_type=f32), lengths
    ).astype(bf16)
    latent_part = jnp.dot(hidden, w_latent, preferred_element_type=f32)
    queries = jnp.dot(hidden, w_query, preferred_element_type=f32).astype(bf16)
    queries = queries.reshape(group_size, local_heads, head_span)
    query_latent = jnp.einsum(
        "shn,hnc->shc", queries[..., :nope_width], w_absorb_key, preferred_element_type=f32
    ).astype(bf16)
    packed = jnp.concatenate(
        [
            query_latent.reshape(group_size, -1),
            queries[..., nope_width:].reshape(group_size, -1),
            *split_float(latent_part),
        ],
        axis=1,
    )
    blocks = [packed[:own_rows]] + [
        shift(packed[s * own_rows : (s + 1) * own_rows], -s, "tp") for s in range(1, tp_count)
    ]
    cut = local_heads * rank
    rope_cut = cut + local_heads * rope_width
    query_latent = jnp.concatenate(
        [b[:, :cut].reshape(own_rows, local_heads, rank) for b in blocks], axis=1
    )
    query_rope = jnp.concatenate(
        [b[:, cut:rope_cut].reshape(own_rows, local_heads, rope_width) for b in blocks], axis=1
    )
    pieces = [join_float(b[:, rope_cut : rope_cut + part], b[:, rope_cut + part :]) for b in blocks]
    columns = []
    for j in range(tp_count):
        column = pieces[0]
        for s in range(1, tp_count):
            column = jnp.where((me + s) % tp_count == j, pieces[s], column)
        columns.append(column)
    new_latent = normalize(jnp.concatenate(columns, axis=1), latent_gain).astype(bf16)
    query_rope = rotate(query_rope.astype(f32), lengths[:, None]).astype(bf16)
    attended = attend(
        query_latent, query_rope, cache_latent, cache_rope, new_latent, new_rope_key, lengths, scaling
    )
    attended = jnp.concatenate(
        [attended[:, :local_heads]]
        + [
            shift(attended[:, s * local_heads : (s + 1) * local_heads], s, "tp")
            for s in range(1, tp_count)
        ]
    )
    head_out = (
        jnp.einsum("shc,hcv->shv", attended, w_absorb_value, preferred_element_type=f32)
        .astype(bf16)
        .reshape(group_size, -1)
    )
    product = jnp.dot(head_out, w_out, preferred_element_type=f32).astype(bf16)
    mixed = product[:own_rows].astype(f32)
    for s in range(1, tp_count):
        mixed = mixed + shift(product[s * own_rows : (s + 1) * own_rows], -s, "tp").astype(f32)
    residual = (tokens.astype(f32) + normalize(mixed, post_gain)).astype(bf16)
    ffn_in = normalize(residual, ffn_gain).astype(bf16)
    dense_gate = jax.nn.sigmoid(jnp.sum(ffn_in.astype(f32) * dense_gate_vector, axis=-1))

    chosen = routes[:, :, None] == jnp.arange(ep_count, dtype=jnp.int32)[None, None, :]
    expert_weight = jnp.sum(jnp.where(chosen, route_weights[:, :, None], 0.0), axis=1)
    w_high, w_low = split_float(expert_weight.T)
    g_high, g_low = split_float(jnp.broadcast_to(dense_gate[None, :], (ep_count, own_rows)))
    extra = jnp.stack([w_high, w_low, g_high, g_low], axis=-1)
    extra = jnp.pad(extra, ((0, 0), (0, 0), (0, 124)))
    outgoing = jnp.concatenate(
        [jnp.broadcast_to(ffn_in[None], (ep_count, own_rows, model_width)), extra], axis=-1
    )
    arrived = lax.all_to_all(outgoing, "ep", split_axis=0, concat_axis=0, tiled=True)
    arrived = arrived.reshape(ep_count * own_rows, -1)
    all_rows = arrived[:, :model_width]
    extra = arrived[:, model_width:].astype(f32)
    row_weight = extra[:, 0:1] + extra[:, 1:2]
    row_gate = extra[:, 2:3] + extra[:, 3:4]
    gate_pre = jnp.dot(all_rows, w_exp_gate[0], preferred_element_type=f32)
    up_proj = jnp.dot(all_rows, w_exp_up[0], preferred_element_type=f32)
    activity = (jax.nn.silu(gate_pre) * up_proj).astype(bf16)
    result = jnp.dot(activity, w_exp_down[0], preferred_element_type=f32).astype(bf16)
    dims = (((1,), (1,)), ((), ()))
    gate_pre = lax.dot_general(all_rows, w_dense_gate, dims, preferred_element_type=f32)
    up_proj = lax.dot_general(all_rows, w_dense_up, dims, preferred_element_type=f32)
    dense_act = (jax.nn.silu(gate_pre) * up_proj).astype(bf16)
    dense_part = jnp.dot(dense_act, w_dense_down, preferred_element_type=f32)
    partial = (row_weight * result.astype(f32) + row_gate * dense_part).astype(bf16)
    returned = lax.all_to_all(
        partial.reshape(ep_count, own_rows, model_width),
        "ep",
        split_axis=0,
        concat_axis=0,
        tiled=True,
    )
    combined = jnp.sum(returned.astype(f32), axis=0)
    output = (residual.astype(f32) + normalize(combined, out_gain)).astype(bf16)
    return (output, new_latent, new_rope_key)


def solution(mesh):
    placed = (
        P(("ep", "tp"), None),
        P(("ep", "tp")),
        P(("ep", "tp"), None, None),
        P(("ep", "tp"), None, None),
        P(),
        P(),
        P(),
        P(),
        P(),
        P(None, "tp"),
        P(),
        P(None, "tp"),
        P("tp", None, None),
        P("tp", None, None),
        P("tp", None),
        P(("ep", "tp"), None),
        P(("ep", "tp"), None),
        P("ep", None, None),
        P("ep", None, None),
        P("ep", None, None),
        P("ep", None),
        P("ep", None),
        P("ep", None),
        P(),
    )
    return jax.shard_map(
        shards,
        mesh=mesh,
        in_specs=placed,
        out_specs=(P(("ep", "tp"), None), P(("ep", "tp"), None), P(("ep", "tp"), None)),
        check_vma=False,
    )
```

```python
import functools

import jax
import jax.numpy as jnp
from jax import lax
from jax.experimental import pallas as pl
from jax.experimental.pallas import tpu as pltpu
from jax.sharding import PartitionSpec as P

epsilon = 1e-06
rope_base = 10000.0
negative = -1e30
f32 = jnp.float32
bf16 = jnp.bfloat16
LANES = 128


def shift(values, step, axis):
    count = lax.axis_size(axis)
    return lax.ppermute(values, axis, [(i, (i + step) % count) for i in range(count)])


def split_float(values):
    high = lax.reduce_precision(values, 8, 7)
    return high.astype(bf16), (values - high).astype(bf16)


def unit_rows(values):
    mean = jnp.mean(values * values, axis=-1, keepdims=True)
    return values * lax.rsqrt(mean + epsilon)


def mm(left, right):
    return jnp.dot(left, right, preferred_element_type=f32)


def mm_t(left, right):
    return lax.dot_general(left, right, (((1,), (1,)), ((), ())), preferred_element_type=f32)


def swap_halves(values):
    half = values.shape[-1] // 2
    return jnp.concatenate([values[:, half:], values[:, :half]], axis=-1)


def silu(values):
    return values / (1.0 + jnp.exp(-values))


def project_body(blocks, heads, *refs):
    tok = refs[:blocks]
    gain, cosine, sine, w_lat, w_rope, w_query, w_key = refs[blocks : blocks + 7]
    outs = refs[blocks + 7 : 2 * blocks + 7]
    rope_key_out, rope_key_own = refs[2 * blocks + 7 :]
    rows = tok[0].shape[0]
    nope, rank = w_key.shape[1:]
    rope = w_rope.shape[0]
    span = nope + rope
    part = w_lat.shape[1]
    values = jnp.concatenate([t[...].astype(f32) for t in tok], axis=0)
    hidden = (unit_rows(values) * gain[...]).astype(bf16)
    queries = mm(hidden, w_query[...])
    latent = mm(hidden, w_lat[...])
    rope_key = mm_t(hidden, w_rope[...])[:rows]
    rope_key = rope_key * cosine[...] + swap_halves(rope_key) * sine[...]
    rope_key_out[...] = rope_key.astype(bf16)
    rope_key_own[...] = rope_key.astype(bf16)
    high = latent.astype(bf16)
    low = (latent - high.astype(f32)).astype(bf16)
    cut = heads * rank
    for h in range(heads):
        nope_part = queries[:, h * span : h * span + nope].astype(bf16)
        absorbed = mm(nope_part, w_key[h]).astype(bf16)
        for s in range(blocks):
            outs[s][:, h * rank : (h + 1) * rank] = absorbed[s * rows : (s + 1) * rows]
    ropes = jnp.concatenate(
        [queries[:, h * span + nope : (h + 1) * span] for h in range(heads)], axis=-1
    ).astype(bf16)
    for s in range(blocks):
        mine = slice(s * rows, (s + 1) * rows)
        start = cut
        for value in (ropes, high, low):
            width = value.shape[1]
            outs[s][:, start : start + width] = value[mine]
            start += width


def prepare_body(lengths, inverse, routes, route_weights, cosine, sine, extra):
    angles = lengths[...].astype(f32) * inverse[...]
    sign = jnp.where(
        lax.broadcasted_iota(jnp.int32, angles.shape, 1) < angles.shape[1] // 2, -1.0, 1.0
    )
    cosine[...] = jnp.cos(angles)
    sine[...] = jnp.sin(angles) * sign
    experts, rows = extra.shape[:2]
    span = -(-experts // LANES) * LANES
    place = lax.broadcasted_iota(jnp.int32, (rows, span), 1)
    table = jnp.zeros((rows, span), f32)
    for k in range(routes.shape[1]):
        one = slice(k, k + 1)
        table = table + jnp.where(place == routes[:, one], route_weights[:, one], 0.0)
    high = table.astype(bf16).astype(f32)
    low = table - high
    lane = lax.broadcasted_iota(jnp.int32, (rows, LANES), 1)
    for e in range(experts):
        one = slice(e, e + 1)
        extra[e] = jnp.where(lane == 0, high[:, one], jnp.where(lane == 1, low[:, one], 0.0))


def attend_body(blocks, heads, scale, *refs):
    packed = refs[:blocks]
    rest = refs[blocks:]
    me_ref, len_ref, cosine, sine, rope_key, gain, cache_lat, cache_rot = rest[:8]
    new_latent_out = rest[8]
    attended = rest[9 : 9 + blocks]
    latents, ropes = rest[9 + blocks :]
    rows = packed[0].shape[0]
    length, rank = cache_lat.shape[1:]
    rope = cache_rot.shape[1]
    span_scale = scale
    part = rank // blocks
    cut = heads * rank
    rope_cut = cut + heads * rope
    me = me_ref[0]
    pieces = []
    for s in range(blocks):
        values = packed[s][...].astype(f32)
        for h in range(heads):
            g = s * heads + h
            latents[:, g, :] = values[:, h * rank : (h + 1) * rank]
            ropes[:, g, :] = values[:, cut + h * rope : cut + (h + 1) * rope]
        pieces.append(
            values[:, rope_cut : rope_cut + part] + values[:, rope_cut + part : rope_cut + 2 * part]
        )
    columns = []
    for j in range(blocks):
        column = pieces[0]
        for s in range(1, blocks):
            column = jnp.where((me + s) % blocks == j, pieces[s], column)
        columns.append(column)
    new_latent = (unit_rows(jnp.concatenate(columns, axis=-1)) * gain[...]).astype(bf16)
    new_latent_out[...] = new_latent
    new_latent = new_latent.astype(f32)
    new_rope = rope_key[...].astype(f32)
    position = lax.broadcasted_iota(jnp.int32, (blocks * heads, length), 1)
    for b in range(rows):
        one = slice(b, b + 1)
        q_lat = latents[b]
        q_rot = ropes[b]
        q_rot = q_rot * cosine[one, :] + swap_halves(q_rot) * sine[one, :]
        q_rot = q_rot.astype(bf16)
        scores = mm_t(q_lat.astype(bf16), cache_lat[b]) + mm(q_rot, cache_rot[b])
        own = jnp.sum(q_lat * new_latent[one], axis=-1, keepdims=True)
        own = own + jnp.sum(q_rot.astype(f32) * new_rope[one], axis=-1, keepdims=True)
        own = own * span_scale
        scores = jnp.where(position < len_ref[b], scores * span_scale, negative)
        top = jnp.maximum(jnp.max(scores, axis=-1, keepdims=True), own)
        weights = jnp.exp(scores - top)
        own = jnp.exp(own - top)
        total = jnp.sum(weights, axis=-1, keepdims=True) + own
        mixed = mm((weights / total).astype(bf16), cache_lat[b])
        own = (own / total).astype(bf16).astype(f32)
        mixed = (mixed + own * new_latent[one]).astype(bf16)
        for s in range(blocks):
            for h in range(heads):
                g = s * heads + h
                attended[s][one, h * rank : (h + 1) * rank] = mixed[g : g + 1]


def heads_body(blocks, heads, *refs):
    attended = refs[:blocks]
    value_t, w_out = refs[blocks : blocks + 2]
    products = refs[blocks + 2 :]
    rows = attended[0].shape[0]
    rank = value_t.shape[2]
    values = jnp.concatenate([a[...].astype(f32) for a in attended], axis=0).astype(bf16)
    pieces = [
        mm_t(values[:, h * rank : (h + 1) * rank], value_t[h]) for h in range(heads)
    ]
    product = mm(jnp.concatenate(pieces, axis=-1).astype(bf16), w_out[...]).astype(bf16)
    for s in range(blocks):
        products[s][...] = product[s * rows : (s + 1) * rows]


def residual_body(blocks, *refs):
    products = refs[:blocks]
    tokens, post_gain, ffn_gain, gate_vec, extra, residual_out, outgoing = refs[blocks:]
    rows = tokens.shape[0]
    mixed = products[0][...].astype(f32)
    for s in range(1, blocks):
        mixed = mixed + products[s][...].astype(f32)
    residual = (tokens[...].astype(f32) + unit_rows(mixed) * post_gain[...]).astype(bf16)
    residual_out[...] = residual
    ffn_in = (unit_rows(residual.astype(f32)) * ffn_gain[...]).astype(bf16)
    logit = jnp.sum(ffn_in.astype(f32) * gate_vec[...], axis=-1, keepdims=True)
    gate = 1.0 / (1.0 + jnp.exp(-logit))
    high = gate.astype(bf16).astype(f32)
    lane = lax.broadcasted_iota(jnp.int32, (rows, LANES), 1)
    gates = jnp.where(lane == 2, high, jnp.where(lane == 3, gate - high, 0.0))
    width = ffn_in.shape[1]
    for e in range(outgoing.shape[0]):
        outgoing[e, :, :width] = ffn_in
        outgoing[e, :, width:] = (extra[e] + gates).astype(bf16)


def hidden_units(rows, gate_w, up_w, product):
    return (silu(product(rows, gate_w[...])) * product(rows, up_w[...])).astype(bf16)


def units_body(arrived, exp_gate, exp_up, exp_down, gate_w, up_w, down_w, out):
    width = exp_gate.shape[0]
    rows = arrived[:, :width]
    extra = arrived[:, width:].astype(f32)
    row_weight = extra[:, 0:1] + extra[:, 1:2]
    row_gate = extra[:, 2:3] + extra[:, 3:4]
    routed = mm(hidden_units(rows, exp_gate, exp_up, mm), exp_down[...]).astype(bf16)
    dense = mm(hidden_units(rows, gate_w, up_w, mm_t), down_w[...])
    out[...] = (row_weight * routed.astype(f32) + row_gate * dense).astype(bf16)


def finish_body(returned, residual, gain, out):
    combined = returned[0].astype(f32)
    for e in range(1, returned.shape[0]):
        combined = combined + returned[e].astype(f32)
    out[...] = (residual[...].astype(f32) + unit_rows(combined) * gain[...]).astype(bf16)


VMEM = pl.BlockSpec(memory_space=pltpu.VMEM)
HBM = pl.BlockSpec(memory_space=pltpu.HBM)
SMEM = pl.BlockSpec(memory_space=pltpu.SMEM)


def call(body, shapes, specs, scratch, flops, limit, name, args):
    return pl.pallas_call(
        body,
        out_shape=[jax.ShapeDtypeStruct(s, t) for s, t in shapes],
        in_specs=specs,
        out_specs=[VMEM] * len(shapes),
        scratch_shapes=scratch,
        cost_estimate=pl.CostEstimate(flops=flops, bytes_accessed=1 << 20, transcendentals=0),
        compiler_params=pltpu.CompilerParams(vmem_limit_bytes=limit << 20),
        name=name,
    )(*args)


def shards(
    tokens,
    lengths,
    cache_latent,
    cache_rope,
    attn_gain,
    latent_gain,
    post_gain,
    ffn_gain,
    out_gain,
    w_latent,
    w_rope_key,
    w_query,
    w_absorb_key,
    w_absorb_value,
    w_out,
    routes,
    route_weights,
    w_exp_gate,
    w_exp_up,
    w_exp_down,
    w_dense_gate,
    w_dense_up,
    w_dense_down,
    dense_gate_vector,
):
    own_rows, model_width = tokens.shape
    tp_count = lax.axis_size("tp")
    ep_count = lax.axis_size("ep")
    rope_width = w_rope_key.shape[1]
    heads, nope_width, rank = w_absorb_key.shape
    part = w_latent.shape[1]
    scale = (nope_width + rope_width) ** (-0.5)
    others = range(1, tp_count)

    rows = [shift(tokens, s, "tp") for s in others]
    value_t = jnp.swapaxes(w_absorb_value, 1, 2)

    half = rope_width // 2
    inverse = rope_base ** (-(jnp.arange(rope_width, dtype=f32) % half) / half)
    cosine, sine, extra = call(
        prepare_body,
        [((own_rows, rope_width), f32)] * 2 + [((ep_count, own_rows, LANES), f32)],
        [VMEM] * 4,
        [],
        1 << 33,
        4,
        "prepare",
        [lengths.reshape(-1, 1), inverse.reshape(1, -1), routes, route_weights],
    )
    packed_width = heads * (rank + rope_width) + 2 * part
    *packed, new_rope_key, rope_key = call(
        functools.partial(project_body, tp_count, heads),
        [((own_rows, packed_width), bf16)] * tp_count + [((own_rows, rope_width), bf16)] * 2,
        [VMEM] * (tp_count + 7),
        [],
        1 << 33,
        6,
        "project",
        [tokens, *rows, attn_gain.reshape(1, -1), cosine, sine, w_latent, w_rope_key.T, w_query, w_absorb_key],
    )
    packed = [packed[0]] + [shift(packed[s], -s, "tp") for s in others]
    me = jnp.full((1,), lax.axis_index("tp"), jnp.int32)
    new_latent, *attended = call(
        functools.partial(attend_body, tp_count, heads, scale),
        [((own_rows, rank), bf16)] + [((own_rows, heads * rank), bf16)] * tp_count,
        [VMEM] * tp_count + [SMEM, SMEM] + [VMEM] * 6,
        [
            pltpu.VMEM((own_rows, tp_count * heads, rank), f32),
            pltpu.VMEM((own_rows, tp_count * heads, rope_width), f32),
        ],
        1 << 33,
        8,
        "attend",
        [*packed, me, lengths, cosine, sine, rope_key, latent_gain.reshape(1, -1), cache_latent, cache_rope],
    )
    attended = [attended[0]] + [shift(attended[s], s, "tp") for s in others]
    products = call(
        functools.partial(heads_body, tp_count, heads),
        [((own_rows, model_width), bf16)] * tp_count,
        [VMEM] * (tp_count + 2),
        [],
        1 << 31,
        4,
        "heads",
        [*attended, value_t, w_out],
    )
    products = [products[0]] + [shift(products[s], -s, "tp") for s in others]
    residual, outgoing = call(
        functools.partial(residual_body, tp_count),
        [
            ((own_rows, model_width), bf16),
            ((ep_count, own_rows, model_width + LANES), bf16),
        ],
        [VMEM] * (tp_count + 5),
        [],
        1 << 31,
        4,
        "residual",
        [*products, tokens, post_gain.reshape(1, -1), ffn_gain.reshape(1, -1), dense_gate_vector.reshape(1, -1), extra],
    )
    arrived = lax.all_to_all(outgoing, "ep", split_axis=0, concat_axis=0, tiled=True)
    (partial,) = call(
        units_body,
        [((ep_count * own_rows, model_width), bf16)],
        [VMEM] * 7,
        [],
        1 << 33,
        12,
        "units",
        [
            arrived.reshape(ep_count * own_rows, -1),
            w_exp_gate[0],
            w_exp_up[0],
            w_exp_down[0],
            w_dense_gate,
            w_dense_up,
            w_dense_down,
        ],
    )
    returned = lax.all_to_all(
        partial.reshape(ep_count, own_rows, model_width),
        "ep",
        split_axis=0,
        concat_axis=0,
        tiled=True,
    )
    (output,) = call(
        finish_body,
        [((own_rows, model_width), bf16)],
        [VMEM] * 3,
        [],
        1 << 30,
        2,
        "finish",
        [returned, residual, out_gain.reshape(1, -1)],
    )
    return (output, new_latent, new_rope_key)


def solution(mesh):
    placed = (
        P(("ep", "tp"), None),
        P(("ep", "tp")),
        P(("ep", "tp"), None, None),
        P(("ep", "tp"), None, None),
        P(),
        P(),
        P(),
        P(),
        P(),
        P(None, "tp"),
        P(),
        P(None, "tp"),
        P("tp", None, None),
        P("tp", None, None),
        P("tp", None),
        P(("ep", "tp"), None),
        P(("ep", "tp"), None),
        P("ep", None, None),
        P("ep", None, None),
        P("ep", None, None),
        P("ep", None),
        P("ep", None),
        P("ep", None),
        P(),
    )
    return jax.shard_map(
        shards,
        mesh=mesh,
        in_specs=placed,
        out_specs=(P(("ep", "tp"), None), P(("ep", "tp"), None), P(("ep", "tp"), None)),
        check_vma=False,
    )
```

```python
import functools
import math

import jax
import jax.numpy as jnp
from jax import lax
from jax.experimental import pallas as pl
from jax.experimental.pallas import tpu as pltpu
from jax.sharding import PartitionSpec as P


epsilon = 1e-06
rope_base = 10000.0
negative = -1e30
f32 = jnp.float32
bf16 = jnp.bfloat16
LANES = 128


def shift(values, step, axis):
    count = lax.axis_size(axis)
    return lax.ppermute(values, axis, [(i, (i + step) % count) for i in range(count)])


def unit_rows(values):
    mean = jnp.mean(values * values, axis=-1, keepdims=True)
    return values * lax.rsqrt(mean + epsilon)


def mm(left, right):
    return jnp.dot(left, right, preferred_element_type=f32)


def mm_t(left, right):
    return lax.dot_general(left, right, (((1,), (1,)), ((), ())), preferred_element_type=f32)


def swap_halves(values):
    half = values.shape[-1] // 2
    return jnp.concatenate([values[:, half:], values[:, :half]], axis=-1)


def silu(values):
    return values / (1.0 + jnp.exp(-values))


def project_body(blocks, heads, *refs):
    tok = refs[:blocks]
    gain, w_lat, w_rope, w_query, w_key = refs[blocks : blocks + 5]
    outs = refs[blocks + 5 : 2 * blocks + 5]
    raw_key = refs[2 * blocks + 5]
    rows = tok[0].shape[0]
    nope, rank = w_key.shape[1:]
    rope = w_rope.shape[0]
    span = nope + rope
    values = jnp.concatenate([t[...].astype(f32) for t in tok], axis=0)
    hidden = (unit_rows(values) * gain[...]).astype(bf16)
    queries = mm(hidden, w_query[...])
    latent = mm(hidden, w_lat[...])
    raw_key[...] = mm_t(hidden, w_rope[...])[:rows]
    high = latent.astype(bf16)
    low = (latent - high.astype(f32)).astype(bf16)
    cut = heads * rank
    for h in range(heads):
        nope_part = queries[:, h * span : h * span + nope].astype(bf16)
        absorbed = mm(nope_part, w_key[h]).astype(bf16)
        for s in range(blocks):
            outs[s][:, h * rank : (h + 1) * rank] = absorbed[s * rows : (s + 1) * rows]
    ropes = jnp.concatenate(
        [queries[:, h * span + nope : (h + 1) * span] for h in range(heads)], axis=-1
    ).astype(bf16)
    for s in range(blocks):
        mine = slice(s * rows, (s + 1) * rows)
        start = cut
        for value in (ropes, high, low):
            width = value.shape[1]
            outs[s][:, start : start + width] = value[mine]
            start += width


def frequency_body(out):
    half = out.shape[1] // 2
    place = lax.rem(lax.broadcasted_iota(jnp.int32, out.shape, 1), half).astype(f32)
    out[...] = jnp.exp(place * (-math.log(rope_base) / half))


def prepare_body(len_ref, inverse, raw_key, cosine, sine, key_out, key_own):
    rows = raw_key.shape[0]
    row = lax.broadcasted_iota(jnp.int32, (rows, 1), 0)
    position = jnp.zeros((rows, 1), f32)
    for b in range(rows):
        position = jnp.where(row == b, len_ref[b].astype(f32), position)
    angles = position * inverse[...]
    lane = lax.broadcasted_iota(jnp.int32, angles.shape, 1)
    cosines = jnp.cos(angles)
    sines = jnp.sin(angles) * jnp.where(lane < angles.shape[1] // 2, -1.0, 1.0)
    cosine[...] = cosines
    sine[...] = sines
    key = raw_key[...]
    key = (key * cosines + swap_halves(key) * sines).astype(bf16)
    key_out[...] = key
    key_own[...] = key


def attend_body(blocks, heads, scale, *refs):
    packed = refs[:blocks]
    rest = refs[blocks:]
    me_ref, len_ref, cosine, sine, rope_key, gain, cache_lat, cache_rot = rest[:8]
    new_latent_out = rest[8]
    attended = rest[9 : 9 + blocks]
    latents, ropes = rest[9 + blocks :]
    rows = packed[0].shape[0]
    length, rank = cache_lat.shape[1:]
    rope = cache_rot.shape[1]
    part = rank // blocks
    cut = heads * rank
    rope_cut = cut + heads * rope
    me = me_ref[0]
    pieces = []
    for s in range(blocks):
        values = packed[s][...].astype(f32)
        for h in range(heads):
            g = s * heads + h
            latents[:, g, :] = values[:, h * rank : (h + 1) * rank]
            ropes[:, g, :] = values[:, cut + h * rope : cut + (h + 1) * rope]
        pieces.append(
            values[:, rope_cut : rope_cut + part] + values[:, rope_cut + part : rope_cut + 2 * part]
        )
    columns = []
    for j in range(blocks):
        column = pieces[0]
        for s in range(1, blocks):
            column = jnp.where((me + s) % blocks == j, pieces[s], column)
        columns.append(column)
    new_latent = (unit_rows(jnp.concatenate(columns, axis=-1)) * gain[...]).astype(bf16)
    new_latent_out[...] = new_latent
    new_latent = new_latent.astype(f32)
    new_rope = rope_key[...].astype(f32)
    position = lax.broadcasted_iota(jnp.int32, (blocks * heads, length), 1)
    scores = []
    owns = []
    for b in range(rows):
        one = slice(b, b + 1)
        q_lat = latents[b]
        q_rot = ropes[b]
        q_rot = q_rot * cosine[one, :] + swap_halves(q_rot) * sine[one, :]
        q_rot = q_rot.astype(bf16)
        score = mm_t(q_lat.astype(bf16), cache_lat[b]) + mm(q_rot, cache_rot[b])
        scores.append(jnp.where(position < len_ref[b], score * scale, negative))
        own = jnp.sum(q_lat * new_latent[one], axis=-1, keepdims=True)
        own = own + jnp.sum(q_rot.astype(f32) * new_rope[one], axis=-1, keepdims=True)
        owns.append(own * scale)
    scores = jnp.concatenate(scores, axis=0)
    own = jnp.concatenate(owns, axis=0)
    top = jnp.maximum(jnp.max(scores, axis=-1, keepdims=True), own)
    weights = jnp.exp(scores - top)
    own = jnp.exp(own - top)
    total = jnp.sum(weights, axis=-1, keepdims=True) + own
    weights = (weights / total).astype(bf16).astype(f32)
    own = (own / total).astype(bf16).astype(f32)
    count = blocks * heads
    for b in range(rows):
        at = slice(b * count, (b + 1) * count)
        mixed = mm(weights[at].astype(bf16), cache_lat[b])
        mixed = (mixed + own[at] * new_latent[b : b + 1]).astype(bf16)
        for s in range(blocks):
            for h in range(heads):
                g = s * heads + h
                attended[s][b : b + 1, h * rank : (h + 1) * rank] = mixed[g : g + 1]


def mix_body(blocks, heads, cores, *refs):
    attended = refs[:blocks]
    core_ref, value_t, w_out = refs[blocks : blocks + 3]
    per_core = heads // cores
    count = (blocks - 1) * heads
    pieces = refs[blocks + 3 : blocks + 3 + count]
    rest = refs[blocks + 3 + count :]
    tokens, post_gain, ffn_gain, gate_vec, routes, route_weights, residual_out, outgoing = rest
    rows, width = tokens.shape
    rank = value_t.shape[1]
    span = value_t.shape[0] // heads
    core = core_ref[0]

    def columns(s, h):
        return attended[s][:, h * rank : (h + 1) * rank]

    outs = [mm_t(columns(0, h), value_t[h * span : (h + 1) * span]) for h in range(heads)]
    product = mm(jnp.concatenate(outs, axis=-1).astype(bf16), w_out[...])
    mixed = product.astype(bf16).astype(f32)
    for s in range(1, blocks):
        group = pieces[(s - 1) * heads : s * heads]
        product = jnp.zeros((rows, width), f32)
        for n, piece in enumerate(group):
            picked = columns(s, n)
            if cores == 2:
                swapped = columns(s, (n + per_core) % heads)
                picked = jnp.where(core == 0, picked.astype(f32), swapped.astype(f32)).astype(bf16)
            one_head = mm_t(picked, piece[:, width:]).astype(bf16)
            product = product + mm(one_head, piece[:, :width])
        mixed = mixed + product.astype(bf16).astype(f32)
    residual = (tokens[...].astype(f32) + unit_rows(mixed) * post_gain[...]).astype(bf16)
    residual_out[...] = residual
    ffn_in = (unit_rows(residual.astype(f32)) * ffn_gain[...]).astype(bf16)
    logit = jnp.sum(ffn_in.astype(f32) * gate_vec[...], axis=-1, keepdims=True)
    gate = 1.0 / (1.0 + jnp.exp(-logit))
    experts, _, total = outgoing.shape
    lane = lax.broadcasted_iota(jnp.int32, (rows, total - width), 1)
    place = jnp.where(lane < experts, lane, lane - experts)
    table = jnp.where(lane >= 2 * experts, gate, 0.0)
    for k in range(routes.shape[1]):
        at = slice(k, k + 1)
        named = jnp.logical_and(place == routes[:, at], lane < 2 * experts)
        table = table + jnp.where(named, route_weights[:, at], 0.0)
    high = table.astype(bf16).astype(f32)
    first = jnp.logical_or(lane < experts, lane == 2 * experts)
    extra = jnp.where(first, high, table - high).astype(bf16)
    for e in range(experts):
        outgoing[e, :, :width] = ffn_in
        outgoing[e, :, width:] = extra


def hidden_units(rows, gate_w, up_w, product):
    return (silu(product(rows, gate_w[...])) * product(rows, up_w[...])).astype(bf16)


def units_body(experts, arrived, exp_gate, exp_up, gate_w, up_w, *outs):
    weight_out, gate_out, routed_act, dense_act = outs
    width = exp_gate.shape[0]
    rows = arrived[:, :width]
    extra = arrived[:, width:].astype(f32)
    lane = lax.broadcasted_iota(jnp.int32, extra.shape, 1)
    mine = lax.axis_index("ep")
    named = jnp.logical_or(lane == mine, lane == mine + experts)
    row_weight = jnp.sum(jnp.where(named, extra, 0.0), axis=-1, keepdims=True)
    named = jnp.logical_or(lane == 2 * experts, lane == 2 * experts + 1)
    row_gate = jnp.sum(jnp.where(named, extra, 0.0), axis=-1, keepdims=True)
    weight_out[...] = row_weight
    gate_out[...] = row_gate
    routed_act[...] = hidden_units(rows, exp_gate, exp_up, mm)
    dense_act[...] = hidden_units(rows, gate_w, up_w, mm_t)


def down_body(row_weight, row_gate, routed_act, dense_act, exp_down, down_w, out):
    routed = mm(routed_act[...], exp_down[...]).astype(bf16)
    dense = mm(dense_act[...], down_w[...])
    out[...] = (row_weight[...] * routed.astype(f32) + row_gate[...] * dense).astype(bf16)


def finish_body(returned, residual, gain, out):
    combined = returned[0].astype(f32)
    for e in range(1, returned.shape[0]):
        combined = combined + returned[e].astype(f32)
    out[...] = (residual[...].astype(f32) + unit_rows(combined) * gain[...]).astype(bf16)


VMEM = pl.BlockSpec(memory_space=pltpu.VMEM)
HBM = pl.BlockSpec(memory_space=pltpu.HBM)
SMEM = pl.BlockSpec(memory_space=pltpu.SMEM)


def call(body, shapes, specs, scratch, flops, limit, args):
    return pl.pallas_call(
        body,
        out_shape=[jax.ShapeDtypeStruct(s, t) for s, t in shapes],
        in_specs=specs,
        out_specs=[VMEM] * len(shapes),
        scratch_shapes=scratch,
        cost_estimate=pl.CostEstimate(flops=flops, bytes_accessed=1 << 20, transcendentals=0),
        compiler_params=pltpu.CompilerParams(vmem_limit_bytes=limit << 20),
    )(*args)


def shards(
    tokens,
    lengths,
    cache_latent,
    cache_rope,
    attn_gain,
    latent_gain,
    post_gain,
    ffn_gain,
    out_gain,
    w_latent,
    w_rope_key,
    w_query,
    w_absorb_key,
    w_absorb_value,
    w_out,
    routes,
    route_weights,
    w_exp_gate,
    w_exp_up,
    w_exp_down,
    w_dense_gate,
    w_dense_up,
    w_dense_down,
    dense_gate_vector,
):
    own_rows, model_width = tokens.shape
    tp_count = lax.axis_size("tp")
    ep_count = lax.axis_size("ep")
    rope_width = w_rope_key.shape[1]
    heads, nope_width, rank = w_absorb_key.shape
    part = w_latent.shape[1]
    scale = (nope_width + rope_width) ** (-0.5)
    others = range(1, tp_count)
    extra_width = -(-(2 * ep_count + 2) // LANES) * LANES

    rows = [shift(tokens, s, "tp") for s in others]
    value_t = jnp.swapaxes(w_absorb_value, 1, 2)
    cores = 2 if ep_count % 2 == 0 and heads % 2 == 0 else 1
    core = lax.axis_index("ep") % cores
    per_core = heads // cores
    v_width = value_t.shape[1]
    flat_t = value_t.reshape(heads * v_width, rank)

    def head_weights(k):
        start = (core * per_core + k) * v_width
        return jnp.concatenate(
            [
                lax.dynamic_slice_in_dim(w_out, start, v_width),
                lax.dynamic_slice_in_dim(flat_t, start, v_width),
            ],
            axis=1,
        )

    shares = [head_weights(k) for k in range(per_core)]

    def swap_cores(values):
        return lax.ppermute(values, "ep", [(i, i ^ 1) for i in range(ep_count)])

    fetched = {}
    for s in others:
        fetched[s, 0] = shift(shares[0], -s, "tp")

    (inverse,) = call(frequency_body, [((1, rope_width), f32)], [], [], 1 << 32, 1, [])
    packed_width = heads * (rank + rope_width) + 2 * part
    *packed, raw_key = call(
        functools.partial(project_body, tp_count, heads),
        [((own_rows, packed_width), bf16)] * tp_count + [((own_rows, rope_width), f32)],
        [VMEM] * (tp_count + 5),
        [],
        1 << 32,
        6,
        [
            tokens,
            *rows,
            attn_gain.reshape(1, -1),
            w_latent,
            w_rope_key.T,
            w_query,
            w_absorb_key,
        ],
    )
    cosine, sine, new_rope_key, rope_key = call(
        prepare_body,
        [((own_rows, rope_width), f32)] * 2 + [((own_rows, rope_width), bf16)] * 2,
        [SMEM] + [VMEM] * 2,
        [],
        1 << 31,
        2,
        [lengths, inverse, raw_key],
    )
    mine = packed[0]
    packed = [mine] + [shift(packed[s], -s, "tp") for s in others]
    for k in range(1, per_core):
        late, _ = lax.optimization_barrier((shares[k], mine))
        for s in others:
            fetched[s, k] = shift(late, -s, "tp")
    pieces = []
    for s in others:
        group = [fetched[s, k] for k in range(per_core)]
        pieces += group
        if cores == 2:
            pieces += [swap_cores(piece) for piece in group]
    me = lax.axis_index("tp").reshape(1)
    new_latent, *attended = call(
        functools.partial(attend_body, tp_count, heads, scale),
        [((own_rows, rank), bf16)] + [((own_rows, heads * rank), bf16)] * tp_count,
        [VMEM] * tp_count + [SMEM, SMEM] + [VMEM] * 6,
        [
            pltpu.VMEM((own_rows, tp_count * heads, rank), f32),
            pltpu.VMEM((own_rows, tp_count * heads, rope_width), f32),
        ],
        1 << 29,
        8,
        [*packed, me, lengths, cosine, sine, rope_key, latent_gain.reshape(1, -1), cache_latent, cache_rope],
    )
    residual, outgoing = call(
        functools.partial(mix_body, tp_count, heads, cores),
        [
            ((own_rows, model_width), bf16),
            ((ep_count, own_rows, model_width + extra_width), bf16),
        ],
        [VMEM] * tp_count + [SMEM] + [VMEM] * (8 + len(pieces)),
        [],
        1 << 32,
        8,
        [*attended, core.reshape(1), flat_t, w_out, *pieces, tokens, post_gain.reshape(1, -1), ffn_gain.reshape(1, -1), dense_gate_vector.reshape(1, -1), routes, route_weights],
    )
    arrived = lax.all_to_all(outgoing, "ep", split_axis=0, concat_axis=0, tiled=True)
    units = call(
        functools.partial(units_body, ep_count),
        [((ep_count * own_rows, 1), f32)] * 2
        + [
            ((ep_count * own_rows, w_exp_gate.shape[2]), bf16),
            ((ep_count * own_rows, w_dense_gate.shape[0]), bf16),
        ],
        [VMEM] * 5,
        [],
        1<<27,
        8,
        [
            arrived.reshape(ep_count * own_rows, -1),
            w_exp_gate[0],
            w_exp_up[0],
            w_dense_gate,
            w_dense_up,
        ],
    )
    (partial,) = call(
        down_body,
        [((ep_count * own_rows, model_width), bf16)],
        [VMEM] * 6,
        [],
        1 << 31,
        6,
        [*units, w_exp_down[0], w_dense_down],
    )
    returned = lax.all_to_all(
        partial.reshape(ep_count, own_rows, model_width),
        "ep",
        split_axis=0,
        concat_axis=0,
        tiled=True,
    )
    (output,) = call(
        finish_body,
        [((own_rows, model_width), bf16)],
        [VMEM] * 3,
        [],
        1 << 30,
        2,
        [returned, residual, out_gain.reshape(1, -1)],
    )
    return (output, new_latent, new_rope_key)


def solution(mesh):
    placed = (
        P(("ep", "tp"), None),
        P(("ep", "tp")),
        P(("ep", "tp"), None, None),
        P(("ep", "tp"), None, None),
        P(),
        P(),
        P(),
        P(),
        P(),
        P(None, "tp"),
        P(),
        P(None, "tp"),
        P("tp", None, None),
        P("tp", None, None),
        P("tp", None),
        P(("ep", "tp"), None),
        P(("ep", "tp"), None),
        P("ep", None, None),
        P("ep", None, None),
        P("ep", None, None),
        P("ep", None),
        P("ep", None),
        P("ep", None),
        P(),
    )
    return jax.shard_map(
        shards,
        mesh=mesh,
        in_specs=placed,
        out_specs=(P(("ep", "tp"), None), P(("ep", "tp"), None), P(("ep", "tp"), None)),
        check_vma=False,
    )
```

```python
import functools
import math

import jax
import jax.numpy as jnp
from jax import lax
from jax.experimental import pallas as pl
from jax.experimental.pallas import tpu as pltpu
from jax.sharding import PartitionSpec as P


epsilon = 1e-06
rope_base = 10000.0
negative = -1e30
f32 = jnp.float32
bf16 = jnp.bfloat16
LANES = 128


def shift(values, step, axis):
    count = lax.axis_size(axis)
    return lax.ppermute(values, axis, [(i, (i + step) % count) for i in range(count)])


def unit_rows(values):
    mean = jnp.mean(values * values, axis=-1, keepdims=True)
    return values * lax.rsqrt(mean + epsilon)


def mm(left, right):
    return jnp.dot(left, right, preferred_element_type=f32)


def mm_t(left, right):
    return lax.dot_general(left, right, (((1,), (1,)), ((), ())), preferred_element_type=f32)


def swap_halves(values):
    half = values.shape[-1] // 2
    return jnp.concatenate([values[:, half:], values[:, :half]], axis=-1)


def silu(values):
    return values / (1.0 + jnp.exp(-values))


def project_body(blocks, heads, *refs):
    tok = refs[:blocks]
    gain, w_lat, w_rope, w_query, w_key = refs[blocks : blocks + 5]
    outs = refs[blocks + 5 : 2 * blocks + 5]
    raw_key = refs[2 * blocks + 5]
    rows = tok[0].shape[0]
    nope, rank = w_key.shape[1:]
    rope = w_rope.shape[0]
    span = nope + rope
    values = jnp.concatenate([t[...].astype(f32) for t in tok], axis=0)
    hidden = (unit_rows(values) * gain[...]).astype(bf16)
    queries = mm(hidden, w_query[...])
    latent = mm(hidden, w_lat[...])
    raw_key[...] = mm_t(hidden, w_rope[...])[:rows]
    high = latent.astype(bf16)
    low = (latent - high.astype(f32)).astype(bf16)
    cut = heads * rank
    for h in range(heads):
        nope_part = queries[:, h * span : h * span + nope].astype(bf16)
        absorbed = mm(nope_part, w_key[h]).astype(bf16)
        for s in range(blocks):
            outs[s][:, h * rank : (h + 1) * rank] = absorbed[s * rows : (s + 1) * rows]
    ropes = jnp.concatenate(
        [queries[:, h * span + nope : (h + 1) * span] for h in range(heads)], axis=-1
    ).astype(bf16)
    for s in range(blocks):
        mine = slice(s * rows, (s + 1) * rows)
        start = cut
        for value in (ropes, high, low):
            width = value.shape[1]
            outs[s][:, start : start + width] = value[mine]
            start += width


def frequency_body(out):
    half = out.shape[1] // 2
    place = lax.rem(lax.broadcasted_iota(jnp.int32, out.shape, 1), half).astype(f32)
    out[...] = jnp.exp(place * (-math.log(rope_base) / half))


def prepare_body(len_ref, inverse, raw_key, cosine, sine, key_out, key_own):
    rows = raw_key.shape[0]
    row = lax.broadcasted_iota(jnp.int32, (rows, 1), 0)
    position = jnp.zeros((rows, 1), f32)
    for b in range(rows):
        position = jnp.where(row == b, len_ref[b].astype(f32), position)
    angles = position * inverse[...]
    lane = lax.broadcasted_iota(jnp.int32, angles.shape, 1)
    cosines = jnp.cos(angles)
    sines = jnp.sin(angles) * jnp.where(lane < angles.shape[1] // 2, -1.0, 1.0)
    cosine[...] = cosines
    sine[...] = sines
    key = raw_key[...]
    key = (key * cosines + swap_halves(key) * sines).astype(bf16)
    key_out[...] = key
    key_own[...] = key


def attend_body(blocks, heads, scale, *refs):
    packed = refs[:blocks]
    rest = refs[blocks:]
    me_ref, len_ref, cosine, sine, rope_key, gain, cache_lat, cache_rot = rest[:8]
    new_latent_out = rest[8]
    attended = rest[9 : 9 + blocks]
    latents, ropes = rest[9 + blocks :]
    rows = packed[0].shape[0]
    length, rank = cache_lat.shape[1:]
    rope = cache_rot.shape[1]
    part = rank // blocks
    cut = heads * rank
    rope_cut = cut + heads * rope
    me = me_ref[0]
    pieces = []
    for s in range(blocks):
        values = packed[s][...].astype(f32)
        for h in range(heads):
            g = s * heads + h
            latents[:, g, :] = values[:, h * rank : (h + 1) * rank]
            ropes[:, g, :] = values[:, cut + h * rope : cut + (h + 1) * rope]
        pieces.append(
            values[:, rope_cut : rope_cut + part] + values[:, rope_cut + part : rope_cut + 2 * part]
        )
    columns = []
    for j in range(blocks):
        column = pieces[0]
        for s in range(1, blocks):
            column = jnp.where((me + s) % blocks == j, pieces[s], column)
        columns.append(column)
    new_latent = (unit_rows(jnp.concatenate(columns, axis=-1)) * gain[...]).astype(bf16)
    new_latent_out[...] = new_latent
    new_latent = new_latent.astype(f32)
    new_rope = rope_key[...].astype(f32)
    position = lax.broadcasted_iota(jnp.int32, (blocks * heads, length), 1)
    scores = []
    owns = []
    for b in range(rows):
        one = slice(b, b + 1)
        q_lat = latents[b]
        q_rot = ropes[b]
        q_rot = q_rot * cosine[one, :] + swap_halves(q_rot) * sine[one, :]
        q_rot = q_rot.astype(bf16)
        score = mm_t(q_lat.astype(bf16), cache_lat[b]) + mm(q_rot, cache_rot[b])
        scores.append(jnp.where(position < len_ref[b], score * scale, negative))
        own = jnp.sum(q_lat * new_latent[one], axis=-1, keepdims=True)
        own = own + jnp.sum(q_rot.astype(f32) * new_rope[one], axis=-1, keepdims=True)
        owns.append(own * scale)
    scores = jnp.concatenate(scores, axis=0)
    own = jnp.concatenate(owns, axis=0)
    top = jnp.maximum(jnp.max(scores, axis=-1, keepdims=True), own)
    weights = jnp.exp(scores - top)
    own = jnp.exp(own - top)
    total = jnp.sum(weights, axis=-1, keepdims=True) + own
    weights = (weights / total).astype(bf16).astype(f32)
    own = (own / total).astype(bf16).astype(f32)
    count = blocks * heads
    for b in range(rows):
        at = slice(b * count, (b + 1) * count)
        mixed = mm(weights[at].astype(bf16), cache_lat[b])
        mixed = (mixed + own[at] * new_latent[b : b + 1]).astype(bf16)
        for s in range(blocks):
            for h in range(heads):
                g = s * heads + h
                attended[s][b : b + 1, h * rank : (h + 1) * rank] = mixed[g : g + 1]


def arrived_product(attended, pieces, numbers, heads, core, cores):
    width = pieces[0].shape[1] - attended.shape[1] // heads
    rank = attended.shape[1] // heads
    per_core = heads // cores
    product = jnp.zeros((attended.shape[0], width), f32)
    for n, piece in zip(numbers, pieces):
        picked = attended[:, n * rank : (n + 1) * rank]
        if cores == 2:
            other = (n + per_core) % heads
            swapped = attended[:, other * rank : (other + 1) * rank]
            picked = jnp.where(core == 0, picked.astype(f32), swapped.astype(f32)).astype(bf16)
        one_head = mm_t(picked, piece[:, width:]).astype(bf16)
        product = product + mm(one_head, piece[:, :width])
    return product


def own_body(blocks, heads, cores, numbers, *refs):
    attended = refs[:blocks]
    core_ref, value_t, w_out = refs[blocks : blocks + 3]
    count = len(numbers)
    pieces = refs[blocks + 3 : blocks + 3 + (blocks - 1) * count]
    sums = refs[blocks + 3 + (blocks - 1) * count :]
    rank = value_t.shape[1]
    span = value_t.shape[0] // heads
    outs = [
        mm_t(
            attended[0][:, h * rank : (h + 1) * rank],
            value_t[h * span : (h + 1) * span],
        )
        for h in range(heads)
    ]
    product = mm(jnp.concatenate(outs, axis=-1).astype(bf16), w_out[...])
    sums[0][...] = product.astype(bf16).astype(f32)
    for s in range(1, blocks):
        mine = pieces[(s - 1) * count : s * count]
        sums[s][...] = arrived_product(attended[s], mine, numbers, heads, core_ref[0], cores)


def mix_body(blocks, heads, cores, numbers, *refs):
    sums = refs[:blocks]
    attended = refs[blocks : 2 * blocks - 1]
    core_ref = refs[2 * blocks - 1]
    count = len(numbers)
    pieces = refs[2 * blocks : 2 * blocks + (blocks - 1) * count]
    rest = refs[2 * blocks + (blocks - 1) * count :]
    tokens, post_gain, ffn_gain, gate_vec, routes, route_weights, residual_out, outgoing = rest
    rows, width = tokens.shape
    mixed = sums[0][...]
    for s in range(1, blocks):
        product = sums[s][...]
        if count:
            late = pieces[(s - 1) * count : s * count]
            product = product + arrived_product(
                attended[s - 1], late, numbers, heads, core_ref[0], cores
            )
        mixed = mixed + product.astype(bf16).astype(f32)
    residual = (tokens[...].astype(f32) + unit_rows(mixed) * post_gain[...]).astype(bf16)
    residual_out[...] = residual
    ffn_in = (unit_rows(residual.astype(f32)) * ffn_gain[...]).astype(bf16)
    logit = jnp.sum(ffn_in.astype(f32) * gate_vec[...], axis=-1, keepdims=True)
    gate = 1.0 / (1.0 + jnp.exp(-logit))
    experts, _, total = outgoing.shape
    lane = lax.broadcasted_iota(jnp.int32, (rows, total - width), 1)
    place = jnp.where(lane < experts, lane, lane - experts)
    table = jnp.where(lane >= 2 * experts, gate, 0.0)
    for k in range(routes.shape[1]):
        at = slice(k, k + 1)
        named = jnp.logical_and(place == routes[:, at], lane < 2 * experts)
        table = table + jnp.where(named, route_weights[:, at], 0.0)
    high = table.astype(bf16).astype(f32)
    first = jnp.logical_or(lane < experts, lane == 2 * experts)
    extra = jnp.where(first, high, table - high).astype(bf16)
    for e in range(experts):
        outgoing[e, :, :width] = ffn_in
        outgoing[e, :, width:] = extra


def hidden_units(rows, gate_w, up_w, product):
    return (silu(product(rows, gate_w[...])) * product(rows, up_w[...])).astype(bf16)


def units_body(experts, arrived, exp_gate, exp_up, gate_w, up_w, *outs):
    weight_out, gate_out, routed_act, dense_act = outs
    width = exp_gate.shape[0]
    rows = arrived[:, :width]
    extra = arrived[:, width:].astype(f32)
    lane = lax.broadcasted_iota(jnp.int32, extra.shape, 1)
    mine = lax.axis_index("ep")
    named = jnp.logical_or(lane == mine, lane == mine + experts)
    row_weight = jnp.sum(jnp.where(named, extra, 0.0), axis=-1, keepdims=True)
    named = jnp.logical_or(lane == 2 * experts, lane == 2 * experts + 1)
    row_gate = jnp.sum(jnp.where(named, extra, 0.0), axis=-1, keepdims=True)
    weight_out[...] = row_weight
    gate_out[...] = row_gate
    routed_act[...] = hidden_units(rows, exp_gate, exp_up, mm)
    dense_act[...] = hidden_units(rows, gate_w, up_w, mm_t)


def down_body(row_weight, row_gate, routed_act, dense_act, exp_down, down_w, out):
    routed = mm(routed_act[...], exp_down[...]).astype(bf16)
    dense = mm(dense_act[...], down_w[...])
    out[...] = (row_weight[...] * routed.astype(f32) + row_gate[...] * dense).astype(bf16)


def finish_body(returned, residual, gain, out):
    combined = returned[0].astype(f32)
    for e in range(1, returned.shape[0]):
        combined = combined + returned[e].astype(f32)
    out[...] = (residual[...].astype(f32) + unit_rows(combined) * gain[...]).astype(bf16)


VMEM = pl.BlockSpec(memory_space=pltpu.VMEM)
HBM = pl.BlockSpec(memory_space=pltpu.HBM)
SMEM = pl.BlockSpec(memory_space=pltpu.SMEM)


def call(body, shapes, specs, scratch, flops, limit, args):
    return pl.pallas_call(
        body,
        out_shape=[jax.ShapeDtypeStruct(s, t) for s, t in shapes],
        in_specs=specs,
        out_specs=[VMEM] * len(shapes),
        scratch_shapes=scratch,
        cost_estimate=pl.CostEstimate(flops=flops, bytes_accessed=1 << 20, transcendentals=0),
        compiler_params=pltpu.CompilerParams(vmem_limit_bytes=limit << 20),
    )(*args)


def shards(
    tokens,
    lengths,
    cache_latent,
    cache_rope,
    attn_gain,
    latent_gain,
    post_gain,
    ffn_gain,
    out_gain,
    w_latent,
    w_rope_key,
    w_query,
    w_absorb_key,
    w_absorb_value,
    w_out,
    routes,
    route_weights,
    w_exp_gate,
    w_exp_up,
    w_exp_down,
    w_dense_gate,
    w_dense_up,
    w_dense_down,
    dense_gate_vector,
):
    own_rows, model_width = tokens.shape
    tp_count = lax.axis_size("tp")
    ep_count = lax.axis_size("ep")
    rope_width = w_rope_key.shape[1]
    heads, nope_width, rank = w_absorb_key.shape
    part = w_latent.shape[1]
    scale = (nope_width + rope_width) ** (-0.5)
    others = range(1, tp_count)
    extra_width = -(-(2 * ep_count + 2) // LANES) * LANES

    rows = [shift(tokens, s, "tp") for s in others]
    value_t = jnp.swapaxes(w_absorb_value, 1, 2)
    cores = 2 if ep_count % 2 == 0 and heads % 2 == 0 else 1
    core = lax.axis_index("ep") % cores
    per_core = heads // cores
    v_width = value_t.shape[1]
    flat_t = value_t.reshape(heads * v_width, rank)

    def head_weights(k):
        start = (core * per_core + k) * v_width
        return jnp.concatenate(
            [
                lax.dynamic_slice_in_dim(w_out, start, v_width),
                lax.dynamic_slice_in_dim(flat_t, start, v_width),
            ],
            axis=1,
        )

    shares = [head_weights(k) for k in range(per_core)]

    def swap_cores(values):
        return lax.ppermute(values, "ep", [(i, i ^ 1) for i in range(ep_count)])

    fetched = {}
    for s in others:
        fetched[s, 0] = shift(shares[0], -s, "tp")

    (inverse,) = call(frequency_body, [((1, rope_width), f32)], [], [], 1 << 32, 1, [])
    packed_width = heads * (rank + rope_width) + 2 * part
    *packed, raw_key = call(
        functools.partial(project_body, tp_count, heads),
        [((own_rows, packed_width), bf16)] * tp_count + [((own_rows, rope_width), f32)],
        [VMEM] * (tp_count + 5),
        [],
        1 << 32,
        6,
        [
            tokens,
            *rows,
            attn_gain.reshape(1, -1),
            w_latent,
            w_rope_key.T,
            w_query,
            w_absorb_key,
        ],
    )
    cosine, sine, new_rope_key, rope_key = call(
        prepare_body,
        [((own_rows, rope_width), f32)] * 2 + [((own_rows, rope_width), bf16)] * 2,
        [SMEM] + [VMEM] * 2,
        [],
        1 << 31,
        2,
        [lengths, inverse, raw_key],
    )
    mine = packed[0]
    packed = [mine] + [shift(packed[s], -s, "tp") for s in others]
    for k in range(1, per_core):
        late, _ = lax.optimization_barrier((shares[k], mine))
        for s in others:
            fetched[s, k] = shift(late, -s, "tp")
    pieces = []
    for s in others:
        group = [fetched[s, k] for k in range(per_core)]
        if cores == 2:
            group += [swap_cores(piece) for piece in group]
        pieces.append(group)
    here = list(range(min(heads, per_core + 1)))
    last = list(range(len(here), heads))
    me = lax.axis_index("tp").reshape(1)
    new_latent, *attended = call(
        functools.partial(attend_body, tp_count, heads, scale),
        [((own_rows, rank), bf16)] + [((own_rows, heads * rank), bf16)] * tp_count,
        [VMEM] * tp_count + [SMEM, SMEM] + [VMEM] * 6,
        [
            pltpu.VMEM((own_rows, tp_count * heads, rank), f32),
            pltpu.VMEM((own_rows, tp_count * heads, rope_width), f32),
        ],
        1 << 29,
        8,
        [*packed, me, lengths, cosine, sine, rope_key, latent_gain.reshape(1, -1), cache_latent, cache_rope],
    )
    core = core.reshape(1)
    sums = call(
        functools.partial(own_body, tp_count, heads, cores, tuple(here)),
        [((own_rows, model_width), f32)] * tp_count,
        [VMEM] * tp_count + [SMEM] + [VMEM] * (2 + (tp_count - 1) * len(here)),
        [],
        1 << 29,
        8,
        [*attended, core, flat_t, w_out, *[g[n] for g in pieces for n in here]],
    )
    residual, outgoing = call(
        functools.partial(mix_body, tp_count, heads, cores, tuple(last)),
        [
            ((own_rows, model_width), bf16),
            ((ep_count, own_rows, model_width + extra_width), bf16),
        ],
        [VMEM] * (2 * tp_count - 1) + [SMEM] + [VMEM] * (6 + (tp_count - 1) * len(last)),
        [],
        1 << 32,
        8,
        [
            *sums,
            *attended[1:],
            core,
            *[g[n] for g in pieces for n in last],
            tokens,
            post_gain.reshape(1, -1),
            ffn_gain.reshape(1, -1),
            dense_gate_vector.reshape(1, -1),
            routes,
            route_weights,
        ],
    )
    arrived = lax.all_to_all(outgoing, "ep", split_axis=0, concat_axis=0, tiled=True)
    units = call(
        functools.partial(units_body, ep_count),
        [((ep_count * own_rows, 1), f32)] * 2
        + [
            ((ep_count * own_rows, w_exp_gate.shape[2]), bf16),
            ((ep_count * own_rows, w_dense_gate.shape[0]), bf16),
        ],
        [VMEM] * 5,
        [],
        1<<27,
        8,
        [
            arrived.reshape(ep_count * own_rows, -1),
            w_exp_gate[0],
            w_exp_up[0],
            w_dense_gate,
            w_dense_up,
        ],
    )
    (partial,) = call(
        down_body,
        [((ep_count * own_rows, model_width), bf16)],
        [VMEM] * 6,
        [],
        1 << 31,
        6,
        [*units, w_exp_down[0], w_dense_down],
    )
    returned = lax.all_to_all(
        partial.reshape(ep_count, own_rows, model_width),
        "ep",
        split_axis=0,
        concat_axis=0,
        tiled=True,
    )
    (output,) = call(
        finish_body,
        [((own_rows, model_width), bf16)],
        [VMEM] * 3,
        [],
        1 << 30,
        2,
        [returned, residual, out_gain.reshape(1, -1)],
    )
    return (output, new_latent, new_rope_key)


def solution(mesh):
    placed = (
        P(("ep", "tp"), None),
        P(("ep", "tp")),
        P(("ep", "tp"), None, None),
        P(("ep", "tp"), None, None),
        P(),
        P(),
        P(),
        P(),
        P(),
        P(None, "tp"),
        P(),
        P(None, "tp"),
        P("tp", None, None),
        P("tp", None, None),
        P("tp", None),
        P(("ep", "tp"), None),
        P(("ep", "tp"), None),
        P("ep", None, None),
        P("ep", None, None),
        P("ep", None, None),
        P("ep", None),
        P("ep", None),
        P("ep", None),
        P(),
    )
    return jax.shard_map(
        shards,
        mesh=mesh,
        in_specs=placed,
        out_specs=(P(("ep", "tp"), None), P(("ep", "tp"), None), P(("ep", "tp"), None)),
        check_vma=False,
    )
```

```python
import functools
import math

import jax
import jax.numpy as jnp
from jax import lax
from jax.experimental import pallas as pl
from jax.experimental.pallas import tpu as pltpu
from jax.sharding import PartitionSpec as P


epsilon = 1e-06
rope_base = 10000.0
negative = -1e30
f32 = jnp.float32
bf16 = jnp.bfloat16
LANES = 128


def shift(values, step, axis):
    count = lax.axis_size(axis)
    return lax.ppermute(values, axis, [(i, (i + step) % count) for i in range(count)])


def unit_rows(values):
    mean = jnp.mean(values * values, axis=-1, keepdims=True)
    return values * lax.rsqrt(mean + epsilon)


def mm(left, right):
    return jnp.dot(left, right, preferred_element_type=f32)


def mm_t(left, right):
    return lax.dot_general(left, right, (((1,), (1,)), ((), ())), preferred_element_type=f32)


def swap_halves(values):
    half = values.shape[-1] // 2
    return jnp.concatenate([values[:, half:], values[:, :half]], axis=-1)


def silu(values):
    return values / (1.0 + jnp.exp(-values))


def project_body(blocks, heads, *refs):
    tok = refs[:blocks]
    gain, w_lat, w_rope, w_query, w_key = refs[blocks : blocks + 5]
    outs = refs[blocks + 5 : 2 * blocks + 5]
    raw_key = refs[2 * blocks + 5]
    rows = tok[0].shape[0]
    nope, rank = w_key.shape[1:]
    rope = w_rope.shape[0]
    span = nope + rope
    values = jnp.concatenate([t[...].astype(f32) for t in tok], axis=0)
    hidden = (unit_rows(values) * gain[...]).astype(bf16)
    queries = mm(hidden, w_query[...])
    latent = mm(hidden, w_lat[...])
    raw_key[...] = mm_t(hidden, w_rope[...])[:rows]
    high = latent.astype(bf16)
    low = (latent - high.astype(f32)).astype(bf16)
    cut = heads * rank
    for h in range(heads):
        nope_part = queries[:, h * span : h * span + nope].astype(bf16)
        absorbed = mm(nope_part, w_key[h]).astype(bf16)
        for s in range(blocks):
            outs[s][:, h * rank : (h + 1) * rank] = absorbed[s * rows : (s + 1) * rows]
    ropes = jnp.concatenate(
        [queries[:, h * span + nope : (h + 1) * span] for h in range(heads)], axis=-1
    ).astype(bf16)
    for s in range(blocks):
        mine = slice(s * rows, (s + 1) * rows)
        start = cut
        for value in (ropes, high, low):
            width = value.shape[1]
            outs[s][:, start : start + width] = value[mine]
            start += width


def frequency_body(out):
    half = out.shape[1] // 2
    place = lax.rem(lax.broadcasted_iota(jnp.int32, out.shape, 1), half).astype(f32)
    out[...] = jnp.exp(place * (-math.log(rope_base) / half))


def prepare_body(lengths, inverse, raw_key, cosine, sine, key_out, position_out):
    rows = raw_key.shape[0]
    shape = (rows, rows)
    same = lax.broadcasted_iota(jnp.int32, shape, 0) == lax.broadcasted_iota(jnp.int32, shape, 1)
    column = jnp.where(same, jnp.broadcast_to(lengths[...].astype(f32), shape), 0.0)
    position = jnp.sum(column, axis=-1, keepdims=True)
    position_out[...] = position
    angles = position * inverse[...]
    lane = lax.broadcasted_iota(jnp.int32, angles.shape, 1)
    cosines = jnp.cos(angles)
    sines = jnp.sin(angles) * jnp.where(lane < angles.shape[1] // 2, -1.0, 1.0)
    cosine[...] = cosines
    sine[...] = sines
    key = raw_key[...]
    key_out[...] = (key * cosines + swap_halves(key) * sines).astype(bf16)


def attend_body(blocks, heads, scale, *refs):
    packed = refs[:blocks]
    rest = refs[blocks:]
    lengths, cosine, sine, rope_key, gain, cache_lat, cache_rot = rest[:7]
    new_latent_out = rest[7]
    attended = rest[8 : 8 + blocks]
    latents, ropes = rest[8 + blocks :]
    rows = packed[0].shape[0]
    length, rank = cache_lat.shape[1:]
    rope = cache_rot.shape[1]
    part = rank // blocks
    cut = heads * rank
    rope_cut = cut + heads * rope
    me = lax.axis_index("tp")
    pieces = []
    for s in range(blocks):
        values = packed[s][...].astype(f32)
        for h in range(heads):
            g = s * heads + h
            latents[:, g, :] = values[:, h * rank : (h + 1) * rank]
            ropes[:, g, :] = values[:, cut + h * rope : cut + (h + 1) * rope]
        pieces.append(
            values[:, rope_cut : rope_cut + part] + values[:, rope_cut + part : rope_cut + 2 * part]
        )
    columns = []
    for j in range(blocks):
        column = pieces[0]
        for s in range(1, blocks):
            column = jnp.where((me + s) % blocks == j, pieces[s], column)
        columns.append(column)
    new_latent = (unit_rows(jnp.concatenate(columns, axis=-1)) * gain[...]).astype(bf16)
    new_latent_out[...] = new_latent
    new_latent = new_latent.astype(f32)
    new_rope = rope_key[...].astype(f32)
    position = lax.broadcasted_iota(jnp.int32, (blocks * heads, length), 1).astype(f32)
    scores = []
    owns = []
    for b in range(rows):
        one = slice(b, b + 1)
        q_lat = latents[b]
        q_rot = ropes[b]
        q_rot = q_rot * cosine[one, :] + swap_halves(q_rot) * sine[one, :]
        q_rot = q_rot.astype(bf16)
        score = mm_t(q_lat.astype(bf16), cache_lat[b]) + mm(q_rot, cache_rot[b])
        scores.append(jnp.where(position < lengths[b : b + 1, :], score * scale, negative))
        own = jnp.sum(q_lat * new_latent[one], axis=-1, keepdims=True)
        own = own + jnp.sum(q_rot.astype(f32) * new_rope[one], axis=-1, keepdims=True)
        owns.append(own * scale)
    scores = jnp.concatenate(scores, axis=0)
    own = jnp.concatenate(owns, axis=0)
    top = jnp.maximum(jnp.max(scores, axis=-1, keepdims=True), own)
    weights = jnp.exp(scores - top)
    own = jnp.exp(own - top)
    total = jnp.sum(weights, axis=-1, keepdims=True) + own
    weights = (weights / total).astype(bf16).astype(f32)
    own = (own / total).astype(bf16).astype(f32)
    count = blocks * heads
    for b in range(rows):
        at = slice(b * count, (b + 1) * count)
        mixed = mm(weights[at].astype(bf16), cache_lat[b])
        mixed = (mixed + own[at] * new_latent[b : b + 1]).astype(bf16)
        for s in range(blocks):
            for h in range(heads):
                g = s * heads + h
                attended[s][b : b + 1, h * rank : (h + 1) * rank] = mixed[g : g + 1]


def arrived_product(attended, pieces, numbers, heads, cores):
    width = pieces[0].shape[1] - attended.shape[1] // heads
    rank = attended.shape[1] // heads
    per_core = heads // cores
    core = lax.axis_index("ep") % cores
    product = jnp.zeros((attended.shape[0], width), f32)
    for n, piece in zip(numbers, pieces):
        picked = attended[:, n * rank : (n + 1) * rank]
        if cores == 2:
            other = (n + per_core) % heads
            swapped = attended[:, other * rank : (other + 1) * rank]
            picked = jnp.where(core == 0, picked.astype(f32), swapped.astype(f32)).astype(bf16)
        one_head = mm_t(picked, piece[:, width:]).astype(bf16)
        product = product + mm(one_head, piece[:, :width])
    return product


def own_body(blocks, heads, cores, numbers, *refs):
    attended = refs[:blocks]
    value_t, w_out = refs[blocks : blocks + 2]
    count = len(numbers)
    pieces = refs[blocks + 2 : blocks + 2 + (blocks - 1) * count]
    sums = refs[blocks + 2 + (blocks - 1) * count :]
    rank = value_t.shape[1]
    span = value_t.shape[0] // heads
    outs = [
        mm_t(
            attended[0][:, h * rank : (h + 1) * rank],
            value_t[h * span : (h + 1) * span],
        )
        for h in range(heads)
    ]
    product = mm(jnp.concatenate(outs, axis=-1).astype(bf16), w_out[...])
    sums[0][...] = product.astype(bf16).astype(f32)
    for s in range(1, blocks):
        mine = pieces[(s - 1) * count : s * count]
        sums[s][...] = arrived_product(attended[s], mine, numbers, heads, cores)


def mix_body(blocks, heads, cores, numbers, *refs):
    sums = refs[:blocks]
    attended = refs[blocks : 2 * blocks - 1]
    count = len(numbers)
    pieces = refs[2 * blocks - 1 : 2 * blocks - 1 + (blocks - 1) * count]
    rest = refs[2 * blocks - 1 + (blocks - 1) * count :]
    tokens, post_gain, ffn_gain, gate_vec, routes, route_weights, residual_out, outgoing = rest
    rows, width = tokens.shape
    mixed = sums[0][...]
    for s in range(1, blocks):
        product = sums[s][...]
        if count:
            late = pieces[(s - 1) * count : s * count]
            product = product + arrived_product(
                attended[s - 1], late, numbers, heads, cores
            )
        mixed = mixed + product.astype(bf16).astype(f32)
    residual = (tokens[...].astype(f32) + unit_rows(mixed) * post_gain[...]).astype(bf16)
    residual_out[...] = residual
    ffn_in = (unit_rows(residual.astype(f32)) * ffn_gain[...]).astype(bf16)
    logit = jnp.sum(ffn_in.astype(f32) * gate_vec[...], axis=-1, keepdims=True)
    gate = 1.0 / (1.0 + jnp.exp(-logit))
    experts, _, total = outgoing.shape
    lane = lax.broadcasted_iota(jnp.int32, (rows, total - width), 1)
    place = jnp.where(lane < experts, lane, lane - experts)
    table = jnp.where(lane >= 2 * experts, gate, 0.0)
    for k in range(routes.shape[1]):
        at = slice(k, k + 1)
        named = jnp.logical_and(place == routes[:, at], lane < 2 * experts)
        table = table + jnp.where(named, route_weights[:, at], 0.0)
    high = table.astype(bf16).astype(f32)
    first = jnp.logical_or(lane < experts, lane == 2 * experts)
    extra = jnp.where(first, high, table - high).astype(bf16)
    for e in range(experts):
        outgoing[e, :, :width] = ffn_in
        outgoing[e, :, width:] = extra


def hidden_units(rows, gate_w, up_w, product):
    return (silu(product(rows, gate_w[...])) * product(rows, up_w[...])).astype(bf16)


def units_body(experts, arrived, exp_gate, exp_up, gate_w, up_w, *outs):
    weight_out, gate_out, routed_act, dense_act = outs
    width = exp_gate.shape[0]
    rows = arrived[:, :width]
    extra = arrived[:, width:].astype(f32)
    lane = lax.broadcasted_iota(jnp.int32, extra.shape, 1)
    mine = lax.axis_index("ep")
    named = jnp.logical_or(lane == mine, lane == mine + experts)
    row_weight = jnp.sum(jnp.where(named, extra, 0.0), axis=-1, keepdims=True)
    named = jnp.logical_or(lane == 2 * experts, lane == 2 * experts + 1)
    row_gate = jnp.sum(jnp.where(named, extra, 0.0), axis=-1, keepdims=True)
    weight_out[...] = row_weight
    gate_out[...] = row_gate
    routed_act[...] = hidden_units(rows, exp_gate, exp_up, mm)
    dense_act[...] = hidden_units(rows, gate_w, up_w, mm_t)


def down_body(row_weight, row_gate, routed_act, dense_act, exp_down, down_w, out):
    routed = mm(routed_act[...], exp_down[...]).astype(bf16)
    dense = mm(dense_act[...], down_w[...])
    out[...] = (row_weight[...] * routed.astype(f32) + row_gate[...] * dense).astype(bf16)


def finish_body(returned, residual, gain, latent, key, out, latent_out, key_out):
    latent_out[...] = latent[...]
    key_out[...] = key[...]
    combined = returned[0].astype(f32)
    for e in range(1, returned.shape[0]):
        combined = combined + returned[e].astype(f32)
    out[...] = (residual[...].astype(f32) + unit_rows(combined) * gain[...]).astype(bf16)


VMEM = pl.BlockSpec(memory_space=pltpu.VMEM)


def call(body, shapes, specs, scratch, flops, limit, args):
    return pl.pallas_call(
        body,
        out_shape=[jax.ShapeDtypeStruct(s, t) for s, t in shapes],
        in_specs=specs,
        out_specs=[VMEM] * len(shapes),
        scratch_shapes=scratch,
        cost_estimate=pl.CostEstimate(flops=flops, bytes_accessed=1 << 20, transcendentals=0),
        compiler_params=pltpu.CompilerParams(vmem_limit_bytes=limit << 20),
    )(*args)


def shards(
    tokens,
    lengths,
    cache_latent,
    cache_rope,
    attn_gain,
    latent_gain,
    post_gain,
    ffn_gain,
    out_gain,
    w_latent,
    w_rope_key,
    w_query,
    w_absorb_key,
    w_absorb_value,
    w_out,
    routes,
    route_weights,
    w_exp_gate,
    w_exp_up,
    w_exp_down,
    w_dense_gate,
    w_dense_up,
    w_dense_down,
    dense_gate_vector,
):
    own_rows, model_width = tokens.shape
    tp_count = lax.axis_size("tp")
    ep_count = lax.axis_size("ep")
    rope_width = w_rope_key.shape[1]
    heads, nope_width, rank = w_absorb_key.shape
    part = w_latent.shape[1]
    scale = (nope_width + rope_width) ** (-0.5)
    others = range(1, tp_count)
    extra_width = -(-(2 * ep_count + 2) // LANES) * LANES

    rows = [shift(tokens, s, "tp") for s in others]
    value_t = jnp.swapaxes(w_absorb_value, 1, 2)
    cores = 2 if ep_count % 2 == 0 and heads % 2 == 0 else 1
    core = lax.axis_index("ep") % cores
    per_core = heads // cores
    v_width = value_t.shape[1]
    flat_t = value_t.reshape(heads * v_width, rank)

    def head_weights(k):
        start = (core * per_core + k) * v_width
        return jnp.concatenate(
            [
                lax.dynamic_slice_in_dim(w_out, start, v_width),
                lax.dynamic_slice_in_dim(flat_t, start, v_width),
            ],
            axis=1,
        )

    shares = [head_weights(k) for k in range(per_core)]

    def swap_cores(values):
        return lax.ppermute(values, "ep", [(i, i ^ 1) for i in range(ep_count)])

    fetched = {}
    for s in others:
        fetched[s, 0] = shift(shares[0], -s, "tp")

    (inverse,) = call(frequency_body, [((1, rope_width), f32)], [], [], 1 << 32, 1, [])
    packed_width = heads * (rank + rope_width) + 2 * part
    *packed, raw_key = call(
        functools.partial(project_body, tp_count, heads),
        [((own_rows, packed_width), bf16)] * tp_count + [((own_rows, rope_width), f32)],
        [VMEM] * (tp_count + 5),
        [],
        1 << 32,
        6,
        [
            tokens,
            *rows,
            attn_gain.reshape(1, -1),
            w_latent,
            w_rope_key.T,
            w_query,
            w_absorb_key,
        ],
    )
    cosine, sine, rope_key, position = call(
        prepare_body,
        [((own_rows, rope_width), f32)] * 2
        + [((own_rows, rope_width), bf16), ((own_rows, 1), f32)],
        [VMEM] * 3,
        [],
        1 << 31,
        2,
        [lengths.reshape(1, -1), inverse, raw_key],
    )
    mine = packed[0]
    packed = [mine] + [shift(packed[s], -s, "tp") for s in others]
    for k in range(1, per_core):
        late, _ = lax.optimization_barrier((shares[k], mine))
        for s in others:
            fetched[s, k] = shift(late, -s, "tp")
    pieces = []
    for s in others:
        group = [fetched[s, k] for k in range(per_core)]
        if cores == 2:
            group += [swap_cores(piece) for piece in group]
        pieces.append(group)
    here = [0] if cores == 1 else [0, per_core]
    last = [n for n in range(heads) if n not in here]
    new_latent, *attended = call(
        functools.partial(attend_body, tp_count, heads, scale),
        [((own_rows, rank), bf16)] + [((own_rows, heads * rank), bf16)] * tp_count,
        [VMEM] * (tp_count + 7),
        [
            pltpu.VMEM((own_rows, tp_count * heads, rank), f32),
            pltpu.VMEM((own_rows, tp_count * heads, rope_width), f32),
        ],
        1 << 29,
        8,
        [*packed, position, cosine, sine, rope_key, latent_gain.reshape(1, -1), cache_latent, cache_rope],
    )
    sums = call(
        functools.partial(own_body, tp_count, heads, cores, tuple(here)),
        [((own_rows, model_width), f32)] * tp_count,
        [VMEM] * (tp_count + 2 + (tp_count - 1) * len(here)),
        [],
        1 << 29,
        8,
        [*attended, flat_t, w_out, *[g[n] for g in pieces for n in here]],
    )
    residual, outgoing = call(
        functools.partial(mix_body, tp_count, heads, cores, tuple(last)),
        [
            ((own_rows, model_width), bf16),
            ((ep_count, own_rows, model_width + extra_width), bf16),
        ],
        [VMEM] * (2 * tp_count + 5 + (tp_count - 1) * len(last)),
        [],
        1 << 32,
        8,
        [
            *sums,
            *attended[1:],
            *[g[n] for g in pieces for n in last],
            tokens,
            post_gain.reshape(1, -1),
            ffn_gain.reshape(1, -1),
            dense_gate_vector.reshape(1, -1),
            routes,
            route_weights,
        ],
    )
    arrived = lax.all_to_all(outgoing, "ep", split_axis=0, concat_axis=0, tiled=True)
    units = call(
        functools.partial(units_body, ep_count),
        [((ep_count * own_rows, 1), f32)] * 2
        + [
            ((ep_count * own_rows, w_exp_gate.shape[2]), bf16),
            ((ep_count * own_rows, w_dense_gate.shape[0]), bf16),
        ],
        [VMEM] * 5,
        [],
        1<<27,
        8,
        [
            arrived.reshape(ep_count * own_rows, -1),
            w_exp_gate[0],
            w_exp_up[0],
            w_dense_gate,
            w_dense_up,
        ],
    )
    (partial,) = call(
        down_body,
        [((ep_count * own_rows, model_width), bf16)],
        [VMEM] * 6,
        [],
        1 << 31,
        6,
        [*units, w_exp_down[0], w_dense_down],
    )
    returned = lax.all_to_all(
        partial.reshape(ep_count, own_rows, model_width),
        "ep",
        split_axis=0,
        concat_axis=0,
        tiled=True,
    )
    output, new_latent, new_rope_key = call(
        finish_body,
        [
            ((own_rows, model_width), bf16),
            ((own_rows, rank), bf16),
            ((own_rows, rope_width), bf16),
        ],
        [VMEM] * 5,
        [],
        1 << 30,
        2,
        [returned, residual, out_gain.reshape(1, -1), new_latent, rope_key],
    )
    return (output, new_latent, new_rope_key)


def solution(mesh):
    placed = (
        P(("ep", "tp"), None),
        P(("ep", "tp")),
        P(("ep", "tp"), None, None),
        P(("ep", "tp"), None, None),
        P(),
        P(),
        P(),
        P(),
        P(),
        P(None, "tp"),
        P(),
        P(None, "tp"),
        P("tp", None, None),
        P("tp", None, None),
        P("tp", None),
        P(("ep", "tp"), None),
        P(("ep", "tp"), None),
        P("ep", None, None),
        P("ep", None, None),
        P("ep", None, None),
        P("ep", None),
        P("ep", None),
        P("ep", None),
        P(),
    )
    return jax.shard_map(
        shards,
        mesh=mesh,
        in_specs=placed,
        out_specs=(P(("ep", "tp"), None), P(("ep", "tp"), None), P(("ep", "tp"), None)),
        check_vma=False,
    )
```

```python
import functools
import math

import jax
import jax.numpy as jnp
from jax import lax
from jax.experimental import pallas as pl
from jax.experimental.pallas import tpu as pltpu
from jax.sharding import PartitionSpec as P


epsilon = 1e-06
rope_base = 10000.0
negative = -1e30
f32 = jnp.float32
bf16 = jnp.bfloat16
LANES = 128


def shift(values, step, axis):
    count = lax.axis_size(axis)
    return lax.ppermute(values, axis, [(i, (i + step) % count) for i in range(count)])


def unit_rows(values):
    mean = jnp.mean(values * values, axis=-1, keepdims=True)
    return values * lax.rsqrt(mean + epsilon)


def mm(left, right):
    return jnp.dot(left, right, preferred_element_type=f32)


def mm_t(left, right):
    return lax.dot_general(left, right, (((1,), (1,)), ((), ())), preferred_element_type=f32)


def swap_halves(values):
    half = values.shape[-1] // 2
    return jnp.concatenate([values[:, half:], values[:, :half]], axis=-1)


def silu(values):
    return values / (1.0 + jnp.exp(-values))


def project_body(blocks, heads, *refs):
    tok = refs[:blocks]
    gain, w_lat, w_rope, w_query, w_key = refs[blocks : blocks + 5]
    outs = refs[blocks + 5 : 2 * blocks + 5]
    raw_key = refs[2 * blocks + 5]
    rows = tok[0].shape[0]
    nope, rank = w_key.shape[1:]
    rope = w_rope.shape[0]
    span = nope + rope
    values = jnp.concatenate([t[...].astype(f32) for t in tok], axis=0)
    hidden = (unit_rows(values) * gain[...]).astype(bf16)
    queries = mm(hidden, w_query[...])
    latent = mm(hidden, w_lat[...])
    raw_key[...] = mm_t(hidden, w_rope[...])[:rows]
    high = latent.astype(bf16)
    low = (latent - high.astype(f32)).astype(bf16)
    cut = heads * rank
    for h in range(heads):
        nope_part = queries[:, h * span : h * span + nope].astype(bf16)
        absorbed = mm(nope_part, w_key[h]).astype(bf16)
        for s in range(blocks):
            outs[s][:, h * rank : (h + 1) * rank] = absorbed[s * rows : (s + 1) * rows]
    ropes = jnp.concatenate(
        [queries[:, h * span + nope : (h + 1) * span] for h in range(heads)], axis=-1
    ).astype(bf16)
    for s in range(blocks):
        mine = slice(s * rows, (s + 1) * rows)
        start = cut
        for value in (ropes, high, low):
            width = value.shape[1]
            outs[s][:, start : start + width] = value[mine]
            start += width


def frequency_body(out):
    half = out.shape[1] // 2
    place = lax.rem(lax.broadcasted_iota(jnp.int32, out.shape, 1), half).astype(f32)
    out[...] = jnp.exp(place * (-math.log(rope_base) / half))


def prepare_body(lengths, inverse, raw_key, cosine, sine, key_out, position_out):
    rows = raw_key.shape[0]
    shape = (rows, rows)
    same = lax.broadcasted_iota(jnp.int32, shape, 0) == lax.broadcasted_iota(jnp.int32, shape, 1)
    column = jnp.where(same, jnp.broadcast_to(lengths[...].astype(f32), shape), 0.0)
    position = jnp.sum(column, axis=-1, keepdims=True)
    position_out[...] = position
    angles = position * inverse[...]
    lane = lax.broadcasted_iota(jnp.int32, angles.shape, 1)
    cosines = jnp.cos(angles)
    sines = jnp.sin(angles) * jnp.where(lane < angles.shape[1] // 2, -1.0, 1.0)
    cosine[...] = cosines
    sine[...] = sines
    key = raw_key[...]
    key_out[...] = (key * cosines + swap_halves(key) * sines).astype(bf16)


def attend_body(blocks, heads, scale, *refs):
    packed = refs[:blocks]
    rest = refs[blocks:]
    lengths, cosine, sine, rope_key, gain, cache_lat, cache_rot = rest[:7]
    new_latent_out = rest[7]
    attended = rest[8 : 8 + blocks]
    latents, ropes = rest[8 + blocks :]
    rows = packed[0].shape[0]
    length, rank = cache_lat.shape[1:]
    rope = cache_rot.shape[1]
    part = rank // blocks
    cut = heads * rank
    rope_cut = cut + heads * rope
    me = lax.axis_index("tp")
    pieces = []
    for s in range(blocks):
        values = packed[s][...].astype(f32)
        for h in range(heads):
            g = s * heads + h
            latents[:, g, :] = values[:, h * rank : (h + 1) * rank]
            ropes[:, g, :] = values[:, cut + h * rope : cut + (h + 1) * rope]
        pieces.append(
            values[:, rope_cut : rope_cut + part] + values[:, rope_cut + part : rope_cut + 2 * part]
        )
    columns = []
    for j in range(blocks):
        column = pieces[0]
        for s in range(1, blocks):
            column = jnp.where((me + s) % blocks == j, pieces[s], column)
        columns.append(column)
    new_latent = (unit_rows(jnp.concatenate(columns, axis=-1)) * gain[...]).astype(bf16)
    new_latent_out[...] = new_latent
    new_latent = new_latent.astype(f32)
    new_rope = rope_key[...].astype(f32)
    position = lax.broadcasted_iota(jnp.int32, (blocks * heads, length), 1).astype(f32)
    scores = []
    owns = []
    for b in range(rows):
        one = slice(b, b + 1)
        q_lat = latents[b]
        q_rot = ropes[b]
        q_rot = q_rot * cosine[one, :] + swap_halves(q_rot) * sine[one, :]
        q_rot = q_rot.astype(bf16)
        score = mm_t(q_lat.astype(bf16), cache_lat[b]) + mm(q_rot, cache_rot[b])
        scores.append(jnp.where(position < lengths[b : b + 1, :], score * scale, negative))
        own = jnp.sum(q_lat * new_latent[one], axis=-1, keepdims=True)
        own = own + jnp.sum(q_rot.astype(f32) * new_rope[one], axis=-1, keepdims=True)
        owns.append(own * scale)
    scores = jnp.concatenate(scores, axis=0)
    own = jnp.concatenate(owns, axis=0)
    top = jnp.maximum(jnp.max(scores, axis=-1, keepdims=True), own)
    weights = jnp.exp(scores - top)
    own = jnp.exp(own - top)
    total = jnp.sum(weights, axis=-1, keepdims=True) + own
    weights = (weights / total).astype(bf16).astype(f32)
    own = (own / total).astype(bf16).astype(f32)
    count = blocks * heads
    for b in range(rows):
        at = slice(b * count, (b + 1) * count)
        mixed = mm(weights[at].astype(bf16), cache_lat[b])
        mixed = (mixed + own[at] * new_latent[b : b + 1]).astype(bf16)
        for s in range(blocks):
            for h in range(heads):
                g = s * heads + h
                attended[s][b : b + 1, h * rank : (h + 1) * rank] = mixed[g : g + 1]


def seen_head(attended, n, heads, cores):
    rank = attended.shape[1] // heads
    picked = attended[:, n * rank : (n + 1) * rank]
    if cores == 2:
        other = (n + heads // cores) % heads
        swapped = attended[:, other * rank : (other + 1) * rank]
        core = lax.axis_index("ep") % cores
        picked = jnp.where(core == 0, picked.astype(f32), swapped.astype(f32)).astype(bf16)
    return picked


def own_body(blocks, heads, cores, numbers, *refs):
    attended = refs[:blocks]
    value_t, w_out = refs[blocks : blocks + 2]
    count = len(numbers)
    pieces = refs[blocks + 2 : blocks + 2 + (blocks - 1) * count]
    outs_at = refs[blocks + 2 + (blocks - 1) * count :]
    sums, later = outs_at[:blocks], outs_at[blocks:]
    rank = value_t.shape[1]
    span = value_t.shape[0] // heads
    outs = [
        mm_t(
            attended[0][:, h * rank : (h + 1) * rank],
            value_t[h * span : (h + 1) * span],
        )
        for h in range(heads)
    ]
    product = mm(jnp.concatenate(outs, axis=-1).astype(bf16), w_out[...])
    sums[0][...] = product.astype(bf16).astype(f32)
    width = w_out.shape[1]
    per_core = heads // cores
    for s in range(1, blocks):
        product = jnp.zeros(sums[s].shape, f32)
        waiting = []
        for n, piece in zip(numbers, pieces[(s - 1) * count : s * count]):
            for k in range(per_core):
                values = piece[:, width + k * rank : width + (k + 1) * rank]
                head_out = mm_t(seen_head(attended[s], n + k, heads, cores), values).astype(bf16)
                if k == 0:
                    product = product + mm(head_out, piece[:, :width])
                else:
                    waiting.append(head_out)
        sums[s][...] = product
        for n, head_out in enumerate(waiting):
            later[s - 1][n] = head_out


def mix_body(blocks, count, *refs):
    sums = refs[:blocks]
    later = refs[blocks : 2 * blocks - 1] if count else ()
    pieces = refs[blocks + len(later) : blocks + len(later) + (blocks - 1) * count]
    rest = refs[blocks + len(later) + (blocks - 1) * count :]
    tokens, post_gain, ffn_gain, gate_vec, routes, route_weights, residual_out, outgoing = rest
    rows, width = tokens.shape
    mixed = sums[0][...]
    for s in range(1, blocks):
        product = sums[s][...]
        for n in range(count):
            product = product + mm(later[s - 1][n], pieces[(s - 1) * count + n][...])
        mixed = mixed + product.astype(bf16).astype(f32)
    residual = (tokens[...].astype(f32) + unit_rows(mixed) * post_gain[...]).astype(bf16)
    residual_out[...] = residual
    ffn_in = (unit_rows(residual.astype(f32)) * ffn_gain[...]).astype(bf16)
    logit = jnp.sum(ffn_in.astype(f32) * gate_vec[...], axis=-1, keepdims=True)
    gate = 1.0 / (1.0 + jnp.exp(-logit))
    experts, _, total = outgoing.shape
    lane = lax.broadcasted_iota(jnp.int32, (rows, total - width), 1)
    place = jnp.where(lane < experts, lane, lane - experts)
    table = jnp.where(lane >= 2 * experts, gate, 0.0)
    for k in range(routes.shape[1]):
        at = slice(k, k + 1)
        named = jnp.logical_and(place == routes[:, at], lane < 2 * experts)
        table = table + jnp.where(named, route_weights[:, at], 0.0)
    high = table.astype(bf16).astype(f32)
    first = jnp.logical_or(lane < experts, lane == 2 * experts)
    extra = jnp.where(first, high, table - high).astype(bf16)
    for e in range(experts):
        outgoing[e, :, :width] = ffn_in
        outgoing[e, :, width:] = extra


def hidden_units(rows, gate_w, up_w, product):
    return (silu(product(rows, gate_w[...])) * product(rows, up_w[...])).astype(bf16)


def units_body(experts, arrived, exp_gate, exp_up, gate_w, up_w, *outs):
    weight_out, gate_out, routed_act, dense_act = outs
    width = exp_gate.shape[0]
    rows = arrived[:, :width]
    extra = arrived[:, width:].astype(f32)
    lane = lax.broadcasted_iota(jnp.int32, extra.shape, 1)
    mine = lax.axis_index("ep")
    named = jnp.logical_or(lane == mine, lane == mine + experts)
    row_weight = jnp.sum(jnp.where(named, extra, 0.0), axis=-1, keepdims=True)
    named = jnp.logical_or(lane == 2 * experts, lane == 2 * experts + 1)
    row_gate = jnp.sum(jnp.where(named, extra, 0.0), axis=-1, keepdims=True)
    weight_out[...] = row_weight
    gate_out[...] = row_gate
    routed_act[...] = hidden_units(rows, exp_gate, exp_up, mm)
    dense_act[...] = hidden_units(rows, gate_w, up_w, mm_t)


def down_body(row_weight, row_gate, routed_act, dense_act, exp_down, down_w, out):
    routed = mm(routed_act[...], exp_down[...]).astype(bf16)
    dense = mm(dense_act[...], down_w[...])
    out[...] = (row_weight[...] * routed.astype(f32) + row_gate[...] * dense).astype(bf16)


def finish_body(returned, residual, gain, latent, key, out, latent_out, key_out):
    latent_out[...] = latent[...]
    key_out[...] = key[...]
    combined = returned[0].astype(f32)
    for e in range(1, returned.shape[0]):
        combined = combined + returned[e].astype(f32)
    out[...] = (residual[...].astype(f32) + unit_rows(combined) * gain[...]).astype(bf16)


VMEM = pl.BlockSpec(memory_space=pltpu.VMEM)


def call(body, shapes, specs, scratch, flops, limit, args):
    return pl.pallas_call(
        body,
        out_shape=[jax.ShapeDtypeStruct(s, t) for s, t in shapes],
        in_specs=specs,
        out_specs=[VMEM] * len(shapes),
        scratch_shapes=scratch,
        cost_estimate=pl.CostEstimate(flops=flops, bytes_accessed=1 << 20, transcendentals=0),
        compiler_params=pltpu.CompilerParams(vmem_limit_bytes=limit << 20),
    )(*args)


def shards(
    tokens,
    lengths,
    cache_latent,
    cache_rope,
    attn_gain,
    latent_gain,
    post_gain,
    ffn_gain,
    out_gain,
    w_latent,
    w_rope_key,
    w_query,
    w_absorb_key,
    w_absorb_value,
    w_out,
    routes,
    route_weights,
    w_exp_gate,
    w_exp_up,
    w_exp_down,
    w_dense_gate,
    w_dense_up,
    w_dense_down,
    dense_gate_vector,
):
    own_rows, model_width = tokens.shape
    tp_count = lax.axis_size("tp")
    ep_count = lax.axis_size("ep")
    rope_width = w_rope_key.shape[1]
    heads, nope_width, rank = w_absorb_key.shape
    part = w_latent.shape[1]
    scale = (nope_width + rope_width) ** (-0.5)
    others = range(1, tp_count)
    extra_width = -(-(2 * ep_count + 2) // LANES) * LANES

    rows = [shift(tokens, s, "tp") for s in others]
    value_t = jnp.swapaxes(w_absorb_value, 1, 2)
    cores = 2 if ep_count % 2 == 0 and heads % 2 == 0 else 1
    core = lax.axis_index("ep") % cores
    per_core = heads // cores
    v_width = value_t.shape[1]
    flat_t = value_t.reshape(heads * v_width, rank)

    def head_weights(k):
        first = core * per_core * v_width
        parts = [lax.dynamic_slice_in_dim(w_out, first + k * v_width, v_width)]
        if k == 0:
            parts += [
                lax.dynamic_slice_in_dim(flat_t, first + n * v_width, v_width)
                for n in range(per_core)
            ]
        return jnp.concatenate(parts, axis=1)

    shares = [head_weights(k) for k in range(per_core)]

    def swap_cores(values):
        return lax.ppermute(values, "ep", [(i, i ^ 1) for i in range(ep_count)])

    fetched = {}
    for s in others:
        fetched[s, 0] = shift(shares[0], -s, "tp")

    (inverse,) = call(frequency_body, [((1, rope_width), f32)], [], [], 1 << 32, 1, [])
    packed_width = heads * (rank + rope_width) + 2 * part
    *packed, raw_key = call(
        functools.partial(project_body, tp_count, heads),
        [((own_rows, packed_width), bf16)] * tp_count + [((own_rows, rope_width), f32)],
        [VMEM] * (tp_count + 5),
        [],
        1 << 32,
        6,
        [
            tokens,
            *rows,
            attn_gain.reshape(1, -1),
            w_latent,
            w_rope_key.T,
            w_query,
            w_absorb_key,
        ],
    )
    cosine, sine, rope_key, position = call(
        prepare_body,
        [((own_rows, rope_width), f32)] * 2
        + [((own_rows, rope_width), bf16), ((own_rows, 1), f32)],
        [VMEM] * 3,
        [],
        1 << 31,
        2,
        [lengths.reshape(1, -1), inverse, raw_key],
    )
    mine = packed[0]
    packed = [mine] + [shift(packed[s], -s, "tp") for s in others]
    for k in range(1, per_core):
        late, _ = lax.optimization_barrier((shares[k], mine))
        for s in others:
            fetched[s, k] = shift(late, -s, "tp")
    pieces = []
    for s in others:
        group = [fetched[s, k] for k in range(per_core)]
        if cores == 2:
            group += [swap_cores(piece) for piece in group]
        pieces.append(group)
    here = [0] if cores == 1 else [0, per_core]
    last = [n for n in range(heads) if n not in here]
    new_latent, *attended = call(
        functools.partial(attend_body, tp_count, heads, scale),
        [((own_rows, rank), bf16)] + [((own_rows, heads * rank), bf16)] * tp_count,
        [VMEM] * (tp_count + 7),
        [
            pltpu.VMEM((own_rows, tp_count * heads, rank), f32),
            pltpu.VMEM((own_rows, tp_count * heads, rope_width), f32),
        ],
        1 << 29,
        8,
        [*packed, position, cosine, sine, rope_key, latent_gain.reshape(1, -1), cache_latent, cache_rope],
    )
    own = call(
        functools.partial(own_body, tp_count, heads, cores, tuple(here)),
        [((own_rows, model_width), f32)] * tp_count
        + [((len(last), own_rows, v_width), bf16)] * (tp_count - 1 if last else 0),
        [VMEM] * (tp_count + 2 + (tp_count - 1) * len(here)),
        [],
        1 << 29,
        8,
        [*attended, flat_t, w_out, *[g[n] for g in pieces for n in here]],
    )
    residual, outgoing = call(
        functools.partial(mix_body, tp_count, len(last)),
        [
            ((own_rows, model_width), bf16),
            ((ep_count, own_rows, model_width + extra_width), bf16),
        ],
        [VMEM] * (len(own) + 6 + (tp_count - 1) * len(last)),
        [],
        1 << 32,
        8,
        [
            *own,
            *[g[n] for g in pieces for n in last],
            tokens,
            post_gain.reshape(1, -1),
            ffn_gain.reshape(1, -1),
            dense_gate_vector.reshape(1, -1),
            routes,
            route_weights,
        ],
    )
    arrived = lax.all_to_all(outgoing, "ep", split_axis=0, concat_axis=0, tiled=True)
    units = call(
        functools.partial(units_body, ep_count),
        [((ep_count * own_rows, 1), f32)] * 2
        + [
            ((ep_count * own_rows, w_exp_gate.shape[2]), bf16),
            ((ep_count * own_rows, w_dense_gate.shape[0]), bf16),
        ],
        [VMEM] * 5,
        [],
        1<<27,
        8,
        [
            arrived.reshape(ep_count * own_rows, -1),
            w_exp_gate[0],
            w_exp_up[0],
            w_dense_gate,
            w_dense_up,
        ],
    )
    (partial,) = call(
        down_body,
        [((ep_count * own_rows, model_width), bf16)],
        [VMEM] * 6,
        [],
        1 << 31,
        6,
        [*units, w_exp_down[0], w_dense_down],
    )
    returned = lax.all_to_all(
        partial.reshape(ep_count, own_rows, model_width),
        "ep",
        split_axis=0,
        concat_axis=0,
        tiled=True,
    )
    output, new_latent, new_rope_key = call(
        finish_body,
        [
            ((own_rows, model_width), bf16),
            ((own_rows, rank), bf16),
            ((own_rows, rope_width), bf16),
        ],
        [VMEM] * 5,
        [],
        1 << 30,
        2,
        [returned, residual, out_gain.reshape(1, -1), new_latent, rope_key],
    )
    return (output, new_latent, new_rope_key)


def solution(mesh):
    placed = (
        P(("ep", "tp"), None),
        P(("ep", "tp")),
        P(("ep", "tp"), None, None),
        P(("ep", "tp"), None, None),
        P(),
        P(),
        P(),
        P(),
        P(),
        P(None, "tp"),
        P(),
        P(None, "tp"),
        P("tp", None, None),
        P("tp", None, None),
        P("tp", None),
        P(("ep", "tp"), None),
        P(("ep", "tp"), None),
        P("ep", None, None),
        P("ep", None, None),
        P("ep", None, None),
        P("ep", None),
        P("ep", None),
        P("ep", None),
        P(),
    )
    return jax.shard_map(
        shards,
        mesh=mesh,
        in_specs=placed,
        out_specs=(P(("ep", "tp"), None), P(("ep", "tp"), None), P(("ep", "tp"), None)),
        check_vma=False,
    )
```

```python
import functools
import math

import jax
import jax.numpy as jnp
from jax import lax
from jax.experimental import pallas as pl
from jax.experimental.pallas import tpu as pltpu
from jax.sharding import PartitionSpec as P


epsilon = 1e-06
rope_base = 10000.0
negative = -1e30
f32 = jnp.float32
bf16 = jnp.bfloat16
LANES = 128


def shift(values, step, axis):
    count = lax.axis_size(axis)
    return lax.ppermute(values, axis, [(i, (i + step) % count) for i in range(count)])


def unit_rows(values):
    mean = jnp.mean(values * values, axis=-1, keepdims=True)
    return values * lax.rsqrt(mean + epsilon)


def mm(left, right):
    return jnp.dot(left, right, preferred_element_type=f32)


def mm_t(left, right):
    return lax.dot_general(left, right, (((1,), (1,)), ((), ())), preferred_element_type=f32)


def swap_halves(values):
    half = values.shape[-1] // 2
    return jnp.concatenate([values[:, half:], values[:, :half]], axis=-1)


def silu(values):
    return values / (1.0 + jnp.exp(-values))


def project_body(blocks, heads, *refs):
    tok = refs[:blocks]
    gain, w_lat, w_rope, w_query, w_key = refs[blocks : blocks + 5]
    outs = refs[blocks + 5 : 2 * blocks + 5]
    raw_key = refs[2 * blocks + 5]
    rows = tok[0].shape[0]
    nope, rank = w_key.shape[1:]
    rope = w_rope.shape[0]
    span = nope + rope
    values = jnp.concatenate([t[...].astype(f32) for t in tok], axis=0)
    hidden = (unit_rows(values) * gain[...]).astype(bf16)
    queries = mm(hidden, w_query[...])
    latent = mm(hidden, w_lat[...])
    raw_key[...] = mm_t(hidden, w_rope[...])[:rows]
    high = latent.astype(bf16)
    low = (latent - high.astype(f32)).astype(bf16)
    cut = heads * rank
    for h in range(heads):
        nope_part = queries[:, h * span : h * span + nope].astype(bf16)
        absorbed = mm(nope_part, w_key[h]).astype(bf16)
        for s in range(blocks):
            outs[s][:, h * rank : (h + 1) * rank] = absorbed[s * rows : (s + 1) * rows]
    ropes = jnp.concatenate(
        [queries[:, h * span + nope : (h + 1) * span] for h in range(heads)], axis=-1
    ).astype(bf16)
    for s in range(blocks):
        mine = slice(s * rows, (s + 1) * rows)
        start = cut
        for value in (ropes, high, low):
            width = value.shape[1]
            outs[s][:, start : start + width] = value[mine]
            start += width


def frequency_body(out):
    half = out.shape[1] // 2
    place = lax.rem(lax.broadcasted_iota(jnp.int32, out.shape, 1), half).astype(f32)
    out[...] = jnp.exp(place * (-math.log(rope_base) / half))


def prepare_body(lengths, inverse, raw_key, cosine, sine, key_out, position_out):
    rows = raw_key.shape[0]
    shape = (rows, rows)
    same = lax.broadcasted_iota(jnp.int32, shape, 0) == lax.broadcasted_iota(jnp.int32, shape, 1)
    column = jnp.where(same, jnp.broadcast_to(lengths[...].astype(f32), shape), 0.0)
    position = jnp.sum(column, axis=-1, keepdims=True)
    position_out[...] = position
    angles = position * inverse[...]
    lane = lax.broadcasted_iota(jnp.int32, angles.shape, 1)
    cosines = jnp.cos(angles)
    sines = jnp.sin(angles) * jnp.where(lane < angles.shape[1] // 2, -1.0, 1.0)
    cosine[...] = cosines
    sine[...] = sines
    key = raw_key[...]
    key_out[...] = (key * cosines + swap_halves(key) * sines).astype(bf16)


def attend_body(blocks, heads, scale, *refs):
    packed = refs[:blocks]
    rest = refs[blocks:]
    lengths, cosine, sine, rope_key, gain, cache_lat, cache_rot = rest[:7]
    new_latent_out = rest[7]
    attended = rest[8 : 8 + blocks]
    latents, ropes = rest[8 + blocks :]
    rows = packed[0].shape[0]
    length, rank = cache_lat.shape[1:]
    rope = cache_rot.shape[1]
    part = rank // blocks
    cut = heads * rank
    rope_cut = cut + heads * rope
    me = lax.axis_index("tp")
    pieces = []
    for s in range(blocks):
        values = packed[s][...].astype(f32)
        for h in range(heads):
            g = s * heads + h
            latents[:, g, :] = values[:, h * rank : (h + 1) * rank]
            ropes[:, g, :] = values[:, cut + h * rope : cut + (h + 1) * rope]
        pieces.append(
            values[:, rope_cut : rope_cut + part] + values[:, rope_cut + part : rope_cut + 2 * part]
        )
    columns = []
    for j in range(blocks):
        column = pieces[0]
        for s in range(1, blocks):
            column = jnp.where((me + s) % blocks == j, pieces[s], column)
        columns.append(column)
    new_latent = (unit_rows(jnp.concatenate(columns, axis=-1)) * gain[...]).astype(bf16)
    new_latent_out[...] = new_latent
    new_latent = new_latent.astype(f32)
    new_rope = rope_key[...].astype(f32)
    position = lax.broadcasted_iota(jnp.int32, (blocks * heads, length), 1).astype(f32)
    scores = []
    owns = []
    for b in range(rows):
        one = slice(b, b + 1)
        q_lat = latents[b]
        q_rot = ropes[b]
        q_rot = q_rot * cosine[one, :] + swap_halves(q_rot) * sine[one, :]
        q_rot = q_rot.astype(bf16)
        score = mm_t(q_lat.astype(bf16), cache_lat[b]) + mm(q_rot, cache_rot[b])
        scores.append(jnp.where(position < lengths[b : b + 1, :], score * scale, negative))
        own = jnp.sum(q_lat * new_latent[one], axis=-1, keepdims=True)
        own = own + jnp.sum(q_rot.astype(f32) * new_rope[one], axis=-1, keepdims=True)
        owns.append(own * scale)
    scores = jnp.concatenate(scores, axis=0)
    own = jnp.concatenate(owns, axis=0)
    top = jnp.maximum(jnp.max(scores, axis=-1, keepdims=True), own)
    weights = jnp.exp(scores - top)
    own = jnp.exp(own - top)
    total = jnp.sum(weights, axis=-1, keepdims=True) + own
    weights = (weights / total).astype(bf16).astype(f32)
    own = (own / total).astype(bf16).astype(f32)
    count = blocks * heads
    for b in range(rows):
        at = slice(b * count, (b + 1) * count)
        mixed = mm(weights[at].astype(bf16), cache_lat[b])
        mixed = (mixed + own[at] * new_latent[b : b + 1]).astype(bf16)
        for s in range(blocks):
            for h in range(heads):
                g = s * heads + h
                attended[s][b : b + 1, h * rank : (h + 1) * rank] = mixed[g : g + 1]


def seen_head(attended, n, heads, cores):
    rank = attended.shape[1] // heads
    picked = attended[:, n * rank : (n + 1) * rank]
    if cores == 2:
        other = (n + heads // cores) % heads
        swapped = attended[:, other * rank : (other + 1) * rank]
        core = lax.axis_index("ep") % cores
        picked = jnp.where(core == 0, picked.astype(f32), swapped.astype(f32)).astype(bf16)
    return picked


def own_body(blocks, heads, cores, numbers, *refs):
    attended = refs[:blocks]
    value_t, w_out = refs[blocks : blocks + 2]
    count = len(numbers)
    pieces = refs[blocks + 2 : blocks + 2 + (blocks - 1) * count]
    outs_at = refs[blocks + 2 + (blocks - 1) * count :]
    sums, later = outs_at[:blocks], outs_at[blocks:]
    rank = value_t.shape[1]
    span = value_t.shape[0] // heads
    outs = [
        mm_t(
            attended[0][:, h * rank : (h + 1) * rank],
            value_t[h * span : (h + 1) * span],
        )
        for h in range(heads)
    ]
    product = mm(jnp.concatenate(outs, axis=-1).astype(bf16), w_out[...])
    sums[0][...] = product.astype(bf16).astype(f32)
    width = w_out.shape[1]
    per_core = heads // cores
    for s in range(1, blocks):
        product = jnp.zeros(sums[s].shape, f32)
        waiting = []
        for n, piece in zip(numbers, pieces[(s - 1) * count : s * count]):
            for k in range(per_core):
                values = piece[:, width + k * rank : width + (k + 1) * rank]
                head_out = mm_t(seen_head(attended[s], n + k, heads, cores), values).astype(bf16)
                if k == 0:
                    product = product + mm(head_out, piece[:, :width])
                else:
                    waiting.append(head_out)
        sums[s][...] = product
        for n, head_out in enumerate(waiting):
            later[s - 1][n] = head_out


def mix_body(blocks, count, *refs):
    sums = refs[:blocks]
    later = refs[blocks : 2 * blocks - 1] if count else ()
    pieces = refs[blocks + len(later) : blocks + len(later) + (blocks - 1) * count]
    rest = refs[blocks + len(later) + (blocks - 1) * count :]
    tokens, post_gain, ffn_gain, gate_vec, routes, route_weights, residual_out, outgoing = rest
    rows, width = tokens.shape
    mixed = sums[0][...]
    for s in range(1, blocks):
        product = sums[s][...]
        for n in range(count):
            product = product + mm(later[s - 1][n], pieces[(s - 1) * count + n][...])
        mixed = mixed + product.astype(bf16).astype(f32)
    residual = (tokens[...].astype(f32) + unit_rows(mixed) * post_gain[...]).astype(bf16)
    residual_out[...] = residual
    ffn_in = (unit_rows(residual.astype(f32)) * ffn_gain[...]).astype(bf16)
    logit = jnp.sum(ffn_in.astype(f32) * gate_vec[...], axis=-1, keepdims=True)
    gate = 1.0 / (1.0 + jnp.exp(-logit))
    experts, _, total = outgoing.shape
    lane = lax.broadcasted_iota(jnp.int32, (rows, total - width), 1)
    place = jnp.where(lane < experts, lane, lane - experts)
    table = jnp.where(lane >= 2 * experts, gate, 0.0)
    for k in range(routes.shape[1]):
        at = slice(k, k + 1)
        named = jnp.logical_and(place == routes[:, at], lane < 2 * experts)
        table = table + jnp.where(named, route_weights[:, at], 0.0)
    high = table.astype(bf16).astype(f32)
    first = jnp.logical_or(lane < experts, lane == 2 * experts)
    extra = jnp.where(first, high, table - high).astype(bf16)
    for e in range(experts):
        outgoing[e, :, :width] = ffn_in
        outgoing[e, :, width:] = extra


def hidden_units(rows, gate_w, up_w, product):
    return (silu(product(rows, gate_w[...])) * product(rows, up_w[...])).astype(bf16)


def units_body(experts, arrived, exp_gate, exp_up, gate_w, up_w, *outs):
    weight_out, gate_out, routed_act, dense_act = outs
    width = exp_gate.shape[0]
    blocks = arrived.shape[0]
    values = jnp.concatenate([arrived[e].astype(f32) for e in range(blocks)], axis=0)
    rows = values[:, :width].astype(bf16)
    extra = values[:, width:]
    lane = lax.broadcasted_iota(jnp.int32, extra.shape, 1)
    mine = lax.axis_index("ep")
    named = jnp.logical_or(lane == mine, lane == mine + experts)
    row_weight = jnp.sum(jnp.where(named, extra, 0.0), axis=-1, keepdims=True)
    named = jnp.logical_or(lane == 2 * experts, lane == 2 * experts + 1)
    row_gate = jnp.sum(jnp.where(named, extra, 0.0), axis=-1, keepdims=True)
    weight_out[...] = row_weight
    gate_out[...] = row_gate
    routed_act[...] = hidden_units(rows, exp_gate, exp_up, mm)
    dense_act[...] = hidden_units(rows, gate_w, up_w, mm_t)


def down_body(row_weight, row_gate, routed_act, dense_act, exp_down, down_w, out):
    routed = mm(routed_act[...], exp_down[...]).astype(bf16)
    dense = mm(dense_act[...], down_w[...])
    total = row_weight[...] * routed.astype(f32) + row_gate[...] * dense
    rows = out.shape[1]
    for e in range(out.shape[0]):
        out[e] = total[e * rows : (e + 1) * rows].astype(bf16)


def finish_body(returned, residual, gain, latent, key, out, latent_out, key_out):
    latent_out[...] = latent[...]
    key_out[...] = key[...]
    combined = returned[0].astype(f32)
    for e in range(1, returned.shape[0]):
        combined = combined + returned[e].astype(f32)
    out[...] = (residual[...].astype(f32) + unit_rows(combined) * gain[...]).astype(bf16)


VMEM = pl.BlockSpec(memory_space=pltpu.VMEM)


def call(body, shapes, specs, scratch, flops, limit, args):
    return pl.pallas_call(
        body,
        out_shape=[jax.ShapeDtypeStruct(s, t) for s, t in shapes],
        in_specs=specs,
        out_specs=[VMEM] * len(shapes),
        scratch_shapes=scratch,
        cost_estimate=pl.CostEstimate(flops=flops, bytes_accessed=1 << 20, transcendentals=0),
        compiler_params=pltpu.CompilerParams(vmem_limit_bytes=limit << 20),
    )(*args)


def shards(
    tokens,
    lengths,
    cache_latent,
    cache_rope,
    attn_gain,
    latent_gain,
    post_gain,
    ffn_gain,
    out_gain,
    w_latent,
    w_rope_key,
    w_query,
    w_absorb_key,
    w_absorb_value,
    w_out,
    routes,
    route_weights,
    w_exp_gate,
    w_exp_up,
    w_exp_down,
    w_dense_gate,
    w_dense_up,
    w_dense_down,
    dense_gate_vector,
):
    own_rows, model_width = tokens.shape
    tp_count = lax.axis_size("tp")
    ep_count = lax.axis_size("ep")
    rope_width = w_rope_key.shape[1]
    heads, nope_width, rank = w_absorb_key.shape
    part = w_latent.shape[1]
    scale = (nope_width + rope_width) ** (-0.5)
    others = range(1, tp_count)
    extra_width = -(-(2 * ep_count + 2) // LANES) * LANES

    rows = [shift(tokens, s, "tp") for s in others]
    value_t = jnp.swapaxes(w_absorb_value, 1, 2)
    cores = 2 if ep_count % 2 == 0 and heads % 2 == 0 else 1
    core = lax.axis_index("ep") % cores
    per_core = heads // cores
    v_width = value_t.shape[1]
    flat_t = value_t.reshape(heads * v_width, rank)

    def head_weights(k):
        first = core * per_core * v_width
        parts = [lax.dynamic_slice_in_dim(w_out, first + k * v_width, v_width)]
        if k == 0:
            parts += [
                lax.dynamic_slice_in_dim(flat_t, first + n * v_width, v_width)
                for n in range(per_core)
            ]
        return jnp.concatenate(parts, axis=1)

    shares = [head_weights(k) for k in range(per_core)]

    def swap_cores(values):
        return lax.ppermute(values, "ep", [(i, i ^ 1) for i in range(ep_count)])

    fetched = {}
    for s in others:
        fetched[s, 0] = shift(shares[0], -s, "tp")

    (inverse,) = call(frequency_body, [((1, rope_width), f32)], [], [], 1 << 32, 1, [])
    packed_width = heads * (rank + rope_width) + 2 * part
    *packed, raw_key = call(
        functools.partial(project_body, tp_count, heads),
        [((own_rows, packed_width), bf16)] * tp_count + [((own_rows, rope_width), f32)],
        [VMEM] * (tp_count + 5),
        [],
        1 << 32,
        6,
        [
            tokens,
            *rows,
            attn_gain.reshape(1, -1),
            w_latent,
            w_rope_key.T,
            w_query,
            w_absorb_key,
        ],
    )
    cosine, sine, rope_key, position = call(
        prepare_body,
        [((own_rows, rope_width), f32)] * 2
        + [((own_rows, rope_width), bf16), ((own_rows, 1), f32)],
        [VMEM] * 3,
        [],
        1 << 31,
        2,
        [lengths.reshape(1, -1), inverse, raw_key],
    )
    mine = packed[0]
    packed = [mine] + [shift(packed[s], -s, "tp") for s in others]
    for k in range(1, per_core):
        late, _ = lax.optimization_barrier((shares[k], mine))
        for s in others:
            fetched[s, k] = shift(late, -s, "tp")
    pieces = []
    for s in others:
        group = [fetched[s, k] for k in range(per_core)]
        if cores == 2:
            group += [swap_cores(piece) for piece in group]
        pieces.append(group)
    here = [0] if cores == 1 else [0, per_core]
    last = [n for n in range(heads) if n not in here]
    new_latent, *attended = call(
        functools.partial(attend_body, tp_count, heads, scale),
        [((own_rows, rank), bf16)] + [((own_rows, heads * rank), bf16)] * tp_count,
        [VMEM] * (tp_count + 7),
        [
            pltpu.VMEM((own_rows, tp_count * heads, rank), f32),
            pltpu.VMEM((own_rows, tp_count * heads, rope_width), f32),
        ],
        1 << 29,
        8,
        [*packed, position, cosine, sine, rope_key, latent_gain.reshape(1, -1), cache_latent, cache_rope],
    )
    own = call(
        functools.partial(own_body, tp_count, heads, cores, tuple(here)),
        [((own_rows, model_width), f32)] * tp_count
        + [((len(last), own_rows, v_width), bf16)] * (tp_count - 1 if last else 0),
        [VMEM] * (tp_count + 2 + (tp_count - 1) * len(here)),
        [],
        1 << 29,
        8,
        [*attended, flat_t, w_out, *[g[n] for g in pieces for n in here]],
    )
    residual, outgoing = call(
        functools.partial(mix_body, tp_count, len(last)),
        [
            ((own_rows, model_width), bf16),
            ((ep_count, own_rows, model_width + extra_width), bf16),
        ],
        [VMEM] * (len(own) + 6 + (tp_count - 1) * len(last)),
        [],
        1 << 32,
        8,
        [
            *own,
            *[g[n] for g in pieces for n in last],
            tokens,
            post_gain.reshape(1, -1),
            ffn_gain.reshape(1, -1),
            dense_gate_vector.reshape(1, -1),
            routes,
            route_weights,
        ],
    )
    arrived = lax.all_to_all(outgoing, "ep", split_axis=0, concat_axis=0, tiled=True)
    units = call(
        functools.partial(units_body, ep_count),
        [((ep_count * own_rows, 1), f32)] * 2
        + [
            ((ep_count * own_rows, w_exp_gate.shape[2]), bf16),
            ((ep_count * own_rows, w_dense_gate.shape[0]), bf16),
        ],
        [VMEM] * 5,
        [],
        1<<27,
        8,
        [
            arrived,
            w_exp_gate[0],
            w_exp_up[0],
            w_dense_gate,
            w_dense_up,
        ],
    )
    (partial,) = call(
        down_body,
        [((ep_count, own_rows, model_width), bf16)],
        [VMEM] * 6,
        [],
        1 << 31,
        6,
        [*units, w_exp_down[0], w_dense_down],
    )
    returned = lax.all_to_all(
        partial,
        "ep",
        split_axis=0,
        concat_axis=0,
        tiled=True,
    )
    output, new_latent, new_rope_key = call(
        finish_body,
        [
            ((own_rows, model_width), bf16),
            ((own_rows, rank), bf16),
            ((own_rows, rope_width), bf16),
        ],
        [VMEM] * 5,
        [],
        1 << 30,
        2,
        [returned, residual, out_gain.reshape(1, -1), new_latent, rope_key],
    )
    return (output, new_latent, new_rope_key)


def solution(mesh):
    placed = (
        P(("ep", "tp"), None),
        P(("ep", "tp")),
        P(("ep", "tp"), None, None),
        P(("ep", "tp"), None, None),
        P(),
        P(),
        P(),
        P(),
        P(),
        P(None, "tp"),
        P(),
        P(None, "tp"),
        P("tp", None, None),
        P("tp", None, None),
        P("tp", None),
        P(("ep", "tp"), None),
        P(("ep", "tp"), None),
        P("ep", None, None),
        P("ep", None, None),
        P("ep", None, None),
        P("ep", None),
        P("ep", None),
        P("ep", None),
        P(),
    )
    return jax.shard_map(
        shards,
        mesh=mesh,
        in_specs=placed,
        out_specs=(P(("ep", "tp"), None), P(("ep", "tp"), None), P(("ep", "tp"), None)),
        check_vma=False,
    )
```
